512 devices in a mesh: sp: 64 (over z, y), tp: 8 (over x, core).
Axes of the slice: x: 4, y: 8, z: 8, core: 2. Of those that a mesh axis runs over, the one named last changes fastest.
Arguments:
- skip_stream_entering: bfloat16 [4096, 2048], P('sp'), may hold values from -6 to 6
- reading_vectors: bfloat16 [4096, 1024], P('sp', 'tp'), may hold values from -6 to 6
- blender_lookup_labels: bfloat16 [4096, 1024], P('sp', 'tp'), may hold values from -6 to 6
- blender_payloads: bfloat16 [4096, 1024], P('sp', 'tp'), may hold values from -6 to 6
- blender_result_valve: bfloat16 [4096, 1024], P('sp', 'tp'), may hold values from -6 to 6
- fading_logits: bfloat16 [2, 4096, 1024], P(None, 'sp', 'tp'), as said below
- amend_speed_logits: bfloat16 [2, 4096, 1024], P(None, 'sp', 'tp'), as said below
- extra_log_fades: float32 [2, 16, 4096], P(None, 'tp', 'sp'), may hold values from -3 to 0
- present_reward_factors: float32 [1024], P('tp'), may hold values from -1.2 to 1.2
- attender_scaling_vector: float32 [1024], P('tp'), may hold values from 0.1 to 1.9
- blender_result_projector: bfloat16 [1024, 2048], P('tp'), may hold values from -0.1875 to 0.1875
- blender_scaling_vector: float32 [2048], replicated, may hold values from 0.1 to 1.9
- perceptron_valve_factors: bfloat16 [2048, 5632], P('sp', 'tp'), may hold values from -0.125 to 0.125
- perceptron_widen_factors: bfloat16 [2048, 5632], P('sp', 'tp'), may hold values from -0.125 to 0.125
- perceptron_shrink_factors: bfloat16 [5632, 2048], P('tp', 'sp'), may hold values from -0.078125 to 0.078125
- closing_scaling_vector: float32 [2048], replicated, may hold values from 0.1 to 1.9
Outputs:
- result: bfloat16 [4096, 2048], P(('sp', 'tp'))
The draws below stay inside these ranges and needn't reach their ends.
Inputs may be any that keep to these rules, and one draw needn't show every extreme that they name: `fading_logits`: decay pre-activations. `amend_speed_logits`: correction-rate pre-activations.
All inputs are finite; a program needn't handle non-finite values.
Results may differ from the reference program's by a relative error of at most 0.02.
Values may be sent and summed in bfloat16 or wider, within the bound.
No kernel may reach another device: no remote copies, remote signals or barrier semaphores. Data moves between devices by JAX's collectives and lax.ppermute only.
A program may use at most 64 MiB of HBM per device.

```python
import math
import jax
import jax.numpy as jnp
from jax import lax

D = 2048
FF = 5632
HEADS = 16
HEAD = 64
TOK_DEV = 64
STRING_LENGTH = 4096
BLENDER_WIDTH = 1024
N_TP = 8


def head_classes(key):
    picked = jax.random.uniform(jax.random.fold_in(key, 101), (2, HEADS), jnp.float32)
    slow_share = 0.5
    mixed_index = jax.random.randint(jax.random.fold_in(key, 102), (2,), 0, HEADS)
    mixed = (jnp.arange(HEADS, dtype=jnp.int32)[None, :] == mixed_index[:, None]).astype(jnp.float32)
    slow = (picked < slow_share).astype(jnp.float32) * (1.0 - mixed)
    return (slow, mixed)


def fast_blocks(key):
    block_count = STRING_LENGTH // TOK_DEV
    phase = jax.random.randint(jax.random.fold_in(key, 103), (2,), 0, 8)
    place = (jnp.arange(block_count, dtype=jnp.int32)[None, :] + phase[:, None]) % 8
    extra = jax.random.randint(jax.random.fold_in(key, 104), (2, block_count), 0, 2)
    return jnp.where(place == 4, 1.0, jnp.where(place == 0, extra.astype(jnp.float32), 0.0))


def draw_fading_logits(key, part):
    slow, mixed = head_classes(key)
    block_count = STRING_LENGTH // TOK_DEV
    quick = fast_blocks(key)
    slow_now = slow[:, None, :] + mixed[:, None, :] * (1.0 - quick[:, :, None])
    slow_now = jnp.broadcast_to(slow_now[:, :, None, :], (2, block_count, TOK_DEV, HEADS)).reshape(2, STRING_LENGTH, HEADS)
    slow_cols = jnp.repeat(slow_now, HEAD, axis=2)
    base_vals = slow_cols * (-math.log(STRING_LENGTH) - 0.2) + (1.0 - slow_cols) * -4.0
    offsets = jax.random.uniform(jax.random.fold_in(key, 11), (2, block_count, 1, HEADS), jnp.float32, -0.7, 0.7)
    offsets = jnp.broadcast_to(offsets, (2, block_count, TOK_DEV, HEADS)).reshape(2, STRING_LENGTH, HEADS)
    offsets = jnp.repeat(offsets, HEAD, axis=2)
    noise_vals = jnp.clip(0.5 * jax.random.normal(jax.random.fold_in(key, 12), (2, STRING_LENGTH, BLENDER_WIDTH), jnp.float32), -1.5, 1.5)
    return (base_vals + offsets + noise_vals).astype(jnp.bfloat16)


def draw_amend_speed_logits(key, part):
    slow, mixed = head_classes(key)
    slow_cols = jnp.repeat(slow + mixed, HEAD, axis=1)
    base_vals = slow_cols * math.log(32.0 / STRING_LENGTH)
    noise_vals = jnp.clip(0.7 * jax.random.normal(jax.random.fold_in(key, 21), (2, STRING_LENGTH, BLENDER_WIDTH), jnp.float32), -2.0, 2.0)
    return (base_vals[:, None, :] + noise_vals).astype(jnp.bfloat16)


def draw_extra_log_fades(key, part):
    spots = jax.random.randint(jax.random.fold_in(key, 31), (2, HEADS, 6), 0, STRING_LENGTH)
    depths = jnp.log(jax.random.uniform(jax.random.fold_in(key, 32), (2, HEADS, 6), jnp.float32, 0.5, 0.8))
    places = jnp.arange(STRING_LENGTH, dtype=jnp.int32)
    hits = (spots[..., None] == places).astype(jnp.float32)
    return jnp.einsum('dhb,dhbt->dht', depths, hits)


def levels(stream_key, dims, pieces, least, top_value):
    def one(dim, shards_of):
        draws = jax.random.uniform(jax.random.fold_in(jax.random.fold_in(stream_key, 6), dim), (shards_of,), jnp.float32, least / len(pieces), top_value / len(pieces))
        return jnp.repeat(jnp.exp(draws), dims[dim] // shards_of).reshape((-1,) + (1,) * (len(dims) - dim - 1))

    factor_of = one(*pieces[0])
    for cut in pieces[1:]:
        factor_of = factor_of * one(*cut)
    return factor_of


def scatter_about(key, dims, scale, most, split=(), kind=jnp.bfloat16):
    level = levels(key, dims, split, -0.22, 0.18) if split else 1.0
    values = jax.random.normal(key, dims, jnp.float32) * scale * level
    return jnp.minimum(jnp.maximum(values, -most), most).astype(kind)


def setup_inputs(seed: int = 0) -> dict:
    key_list = jax.random.split(jax.random.key(seed), 17)
    return {
        "skip_stream_entering": scatter_about(key_list[0], (STRING_LENGTH, D), 1.0, 6.0, ((0, 64),)),
        "reading_vectors": scatter_about(key_list[1], (STRING_LENGTH, BLENDER_WIDTH), 1.0, 6.0, ((0, 64), (1, 8))),
        "blender_lookup_labels": scatter_about(key_list[2], (STRING_LENGTH, BLENDER_WIDTH), 1.0, 6.0, ((0, 64), (1, 8))),
        "blender_payloads": scatter_about(key_list[3], (STRING_LENGTH, BLENDER_WIDTH), 1.0, 6.0, ((0, 64), (1, 8))),
        "blender_result_valve": scatter_about(key_list[4], (STRING_LENGTH, BLENDER_WIDTH), 1.0, 6.0, ((0, 64), (1, 8))),
        "fading_logits": draw_fading_logits(jax.random.fold_in(key_list[16], 71), 0),
        "amend_speed_logits": draw_amend_speed_logits(jax.random.fold_in(key_list[16], 71), 0),
        "extra_log_fades": draw_extra_log_fades(jax.random.fold_in(key_list[16], 71), 0),
        "present_reward_factors": scatter_about(key_list[8], (BLENDER_WIDTH,), 0.2, 1.2, ((0, 8),), jnp.float32),
        "attender_scaling_vector": jnp.clip(1.0 + 0.18 * jax.random.normal(key_list[9], (BLENDER_WIDTH,), jnp.float32), 0.1, 1.9),
        "blender_result_projector": scatter_about(key_list[10], (BLENDER_WIDTH, D), BLENDER_WIDTH ** -0.5, 0.1875, ((0, 8),)),
        "blender_scaling_vector": jnp.clip(1.0 + 0.18 * jax.random.normal(key_list[11], (D,), jnp.float32), 0.1, 1.9),
        "perceptron_valve_factors": scatter_about(key_list[12], (D, FF), D ** -0.5, 0.125, ((0, 64), (1, 8))),
        "perceptron_widen_factors": scatter_about(key_list[13], (D, FF), D ** -0.5, 0.125, ((0, 64), (1, 8))),
        "perceptron_shrink_factors": scatter_about(key_list[14], (FF, D), FF ** -0.5, 0.078125, ((0, 8), (1, 64))),
        "closing_scaling_vector": jnp.clip(1.0 + 0.18 * jax.random.normal(key_list[15], (D,), jnp.float32), 0.1, 1.9),
    }


RESIDUAL_SCALE = 2.0 ** 0.25
NORM_EPS = 1e-05
GROUP_EPS = 0.00064
KEY_EPS = 1e-06
PRECISE = lax.Precision.HIGHEST

def layer_norm(summand, gain_vec):
    center = lax.optimization_barrier(jnp.mean(summand, -1, keepdims=True))
    spread = lax.optimization_barrier(jnp.mean(jnp.square(summand - center), -1, keepdims=True))
    return (summand - center) * lax.rsqrt(spread + NORM_EPS) * gain_vec

def wire_round(tensor):
    return lax.optimization_barrier(tensor.astype(jnp.bfloat16)).astype(jnp.float32)

def direction_scan(entire_asking_lines, decays, stored_label_lines, payload_line_slab, erase_keys, refills):

    def advance(state_mat, inputs):
        query_vec, decay_vec, write_key, value_vec, erase_vec, refill_vec = inputs
        erased = jnp.einsum('hij,hj->hi', state_mat, erase_vec, precision=PRECISE)
        state_mat = state_mat * decay_vec[:, None, :] + erased[:, :, None] * refill_vec[:, None, :] + value_vec[:, :, None] * write_key[:, None, :]
        return (state_mat, jnp.einsum('hij,hj->hi', state_mat, query_vec, precision=PRECISE))
    start_state = jnp.zeros((HEADS, HEAD, HEAD), jnp.float32)
    _, outputs = lax.scan(advance, start_state, (entire_asking_lines, decays, stored_label_lines, payload_line_slab, erase_keys, refills))
    return outputs

def reference(skip_stream_entering, reading_vectors, blender_lookup_labels, blender_payloads, blender_result_valve, fading_logits, amend_speed_logits, extra_log_fades, present_reward_factors, attender_scaling_vector, blender_result_projector, blender_scaling_vector, perceptron_valve_factors, perceptron_widen_factors, perceptron_shrink_factors, closing_scaling_vector):

    def split_attenders(tensor):
        return tensor.reshape(tensor.shape[:-1] + (HEADS, HEAD))

    def flipped(tensor):
        return jnp.flip(tensor, 0)
    entire_asking_lines = split_attenders(reading_vectors.astype(jnp.float32))
    key_rows = split_attenders(blender_lookup_labels.astype(jnp.float32))
    payload_line_slab = split_attenders(blender_payloads.astype(jnp.float32))
    key_square = lax.optimization_barrier(jnp.sum(key_rows * key_rows, -1, keepdims=True))
    unit_keys = key_rows * lax.rsqrt(key_square + KEY_EPS)
    fading_log_amount = split_attenders(-jnp.exp(-jax.nn.softplus(-fading_logits.astype(jnp.float32)) - 0.5)) + jnp.swapaxes(extra_log_fades, 1, 2)[..., None]
    decays = jnp.exp(fading_log_amount)
    icl_rates = split_attenders(jax.nn.sigmoid(amend_speed_logits.astype(jnp.float32)))
    stored_label_lines = key_rows[None] * icl_rates
    refills = unit_keys[None] * icl_rates
    forward = direction_scan(entire_asking_lines, decays[0], stored_label_lines[0], payload_line_slab, -unit_keys, refills[0])
    backward = flipped(direction_scan(flipped(entire_asking_lines), flipped(decays[1]), flipped(stored_label_lines[1]), flipped(payload_line_slab), flipped(-unit_keys), flipped(refills[1])))
    summed = forward + backward
    center = lax.optimization_barrier(jnp.mean(summed, -1, keepdims=True))
    spread = lax.optimization_barrier(jnp.mean(jnp.square(summed - center), -1, keepdims=True))
    rescaled_lines = (summed - center) * lax.rsqrt(spread + GROUP_EPS) * split_attenders(attender_scaling_vector)
    present_reward_summand = lax.optimization_barrier(jnp.sum(entire_asking_lines * (stored_label_lines[0] + stored_label_lines[1]) * split_attenders(present_reward_factors), -1, keepdims=True)) * payload_line_slab
    merged_attender_lines = ((rescaled_lines + present_reward_summand) * split_attenders(blender_result_valve.astype(jnp.float32))).reshape(STRING_LENGTH, BLENDER_WIDTH)
    merged_attender_lines = merged_attender_lines.astype(jnp.bfloat16)
    group_cols = BLENDER_WIDTH // N_TP
    mixsum = jnp.zeros((STRING_LENGTH, D), jnp.float32)
    for index in range(N_TP):
        partial_mix = jnp.dot(merged_attender_lines[:, index * group_cols:(index + 1) * group_cols], blender_result_projector[index * group_cols:(index + 1) * group_cols], preferred_element_type=jnp.float32)
        mixsum = mixsum + wire_round(partial_mix)
    middle = layer_norm(RESIDUAL_SCALE * skip_stream_entering.astype(jnp.float32) + mixsum, blender_scaling_vector).astype(jnp.bfloat16)
    group_units = FF // N_TP

    def ffn_block(block_rows):
        gate_pre = jnp.dot(block_rows, perceptron_valve_factors, preferred_element_type=jnp.float32)
        up_pre = jnp.dot(block_rows, perceptron_widen_factors, preferred_element_type=jnp.float32)
        inner_act = (jax.nn.silu(gate_pre) * up_pre).astype(jnp.bfloat16)
        downsum = jnp.zeros((block_rows.shape[0], D), jnp.float32)
        for index in range(N_TP):
            partial_down = jnp.dot(inner_act[:, index * group_units:(index + 1) * group_units], perceptron_shrink_factors[index * group_units:(index + 1) * group_units], preferred_element_type=jnp.float32)
            downsum = downsum + wire_round(partial_down)
        return layer_norm(RESIDUAL_SCALE * block_rows.astype(jnp.float32) + downsum, closing_scaling_vector).astype(jnp.bfloat16)
    blocked = lax.map(ffn_block, middle.reshape(STRING_LENGTH // TOK_DEV, TOK_DEV, D))
    return blocked.reshape(STRING_LENGTH, D)
```

```python
import functools
import math

import jax
import jax.numpy as jnp
from jax import lax
from jax.experimental import pallas as pl
from jax.experimental.pallas import tpu as pltpu
from jax.sharding import Mesh
from jax.sharding import PartitionSpec as P

Y = ("yh", "yl")
SP = ("z", "yh", "yl")
SP_TP = ("z", "yh", "yl", "tp")
PEERS = ("yl", "tp")

RESIDUAL_SCALE = 2.0**0.25
NORM_EPS = 1e-05
GROUP_EPS = 0.00064
KEY_EPS = 1e-06
TOK = 64
HEAD = 64
WIDE = 128
SUB = 16
UNITS = 704
PART = 384
D = 2048
F32 = jnp.float32
BF16 = jnp.bfloat16


def iota(shape, dim):
    return lax.broadcasted_iota(jnp.int32, shape, dim)


def dot(a, b):
    return jnp.dot(a, b, preferred_element_type=F32, precision=lax.Precision.HIGHEST)


def dot_nt(a, b):
    return lax.dot_general(
        a, b, (((1,), (1,)), ((), ())), preferred_element_type=F32, precision=lax.Precision.HIGHEST
    )


def dot_tn(a, b):
    return lax.dot_general(
        a, b, (((0,), (0,)), ((), ())), preferred_element_type=F32, precision=lax.Precision.HIGHEST
    )


def low_half(shape):
    return (iota(shape, len(shape) - 1) % WIDE) < HEAD


def by_head(x):
    low = low_half(x.shape)
    return jnp.concatenate([jnp.where(low, x, 0.0), jnp.where(low, 0.0, x)], axis=0)


def joined_heads(x):
    return x[:HEAD] + x[HEAD:]


def head_ones():
    return ((iota((WIDE, WIDE), 0) // HEAD) == (iota((WIDE, WIDE), 1) // HEAD)).astype(F32)


def head_eye():
    return (iota((HEAD, WIDE), 0) == iota((HEAD, WIDE), 1) % HEAD).astype(F32)


def sigmoid(x):
    return 1.0 / (1.0 + jnp.exp(-x))


def unit_lower_inverse(a):
    row, col = iota((WIDE, WIDE), 0), iota((WIDE, WIDE), 1)
    eye = (row == col).astype(F32)
    near = jnp.where(row // 8 == col // 8, a, 0.0)
    second = dot(near, near)
    fourth = dot(second, second)
    inverse = eye - near + second - dot(near, second)
    inverse = inverse + dot(inverse, fourth)
    for size in (8, 16, 32):
        across = (row // (2 * size) == col // (2 * size)) & (row // size != col // size)
        inverse = inverse - dot(inverse, dot(jnp.where(across, a, 0.0), inverse))
    return inverse


def one_way(back, reads, unit, keys, values, log_decay, rate):
    refill, write = unit * rate, keys * rate
    row, col = iota((TOK, TOK), 0), iota((TOK, TOK), 1)
    reach = (col >= row) if back else (col <= row)
    upto = dot(reach.astype(F32), log_decay)
    ahead = upto - log_decay
    whole = upto[:1] if back else upto[TOK - 1 :]
    low = low_half((SUB, WIDE))
    first, second = [], []
    for block in range(TOK // SUB):
        rows = slice(block * SUB, (block + 1) * SUB)
        edge = (block + 1) * SUB - 1 if back else block * SUB
        start = ahead[edge : edge + 1]
        scale = jnp.exp(jnp.minimum(start - upto, 60.0))
        erase_keys, write_keys = refill * scale, write * scale
        erased = unit[rows] * jnp.exp(ahead[rows] - start)
        read = reads[rows] * jnp.exp(upto[rows] - start)
        first.append(
            dot_nt(
                jnp.concatenate([jnp.where(low, erased, 0.0), jnp.where(low, read, 0.0)], axis=0),
                jnp.concatenate([erase_keys, write_keys], axis=0),
            )
        )
        second.append(
            dot_nt(
                jnp.concatenate([jnp.where(low, 0.0, erased), jnp.where(low, 0.0, read)], axis=0),
                jnp.concatenate([write_keys, erase_keys], axis=0),
            )
        )
    row, col = iota((TOK, WIDE), 0), iota((TOK, WIDE), 1) % HEAD
    past = (col > row) if back else (col < row)
    seen = (col >= row) if back else (col <= row)
    low = low_half((TOK, WIDE))

    def pieces(kept, lo):
        one = jnp.concatenate([part[lo : lo + SUB] for part in first], axis=0)
        two = jnp.concatenate([part[lo : lo + SUB] for part in second], axis=0)
        one, two = jnp.where(kept, one, 0.0), jnp.where(kept, two, 0.0)
        same = jnp.concatenate([jnp.where(low, one, 0.0), jnp.where(low, 0.0, two)], axis=0)
        other = jnp.concatenate([jnp.where(low, 0.0, one), jnp.where(low, two, 0.0)], axis=0)
        return same, other

    erase_erase, erase_write = pieces(past, 0)
    read_erase, read_write = pieces(seen, SUB)
    straight = by_head(values)
    crossed = jnp.concatenate([straight[TOK:], straight[:TOK]], axis=0)
    asked = jnp.concatenate([dot(erase_write, crossed), by_head(unit * jnp.exp(ahead))], axis=1)
    erased = -dot(unit_lower_inverse(erase_erase), asked)
    out = dot(read_erase, erased) + jnp.concatenate(
        [dot(read_write, crossed), by_head(reads * jnp.exp(upto))], axis=1
    )
    left = jnp.exp(whole - upto)
    state = dot_tn(by_head(refill * left), erased)
    state = joined_heads(state) + jnp.concatenate(
        [
            joined_heads(dot_tn(by_head(write * left), straight)),
            head_eye() * jnp.exp(whole),
        ],
        axis=1,
    )
    return joined_heads(out), state


def mixer_local(reads_ref, keys_ref, values_ref, fades_ref, rates_ref, extra_ref, send_ref, out_ref):
    reads, keys = reads_ref[...].astype(F32), keys_ref[...].astype(F32)
    values = values_ref[...].astype(F32)
    unit = keys * lax.rsqrt(dot(keys * keys, head_ones()) + KEY_EPS)
    lanes_of = (iota((2, WIDE), 1) // HEAD == iota((2, WIDE), 0)).astype(F32)
    for way in range(2):
        log_decay = -math.exp(-0.5) * sigmoid(fades_ref[way].astype(F32)) + dot_tn(
            extra_ref[way], lanes_of
        )
        rate = sigmoid(rates_ref[way].astype(F32))
        out, state = one_way(way == 1, reads, unit, keys, values, log_decay, rate)
        out_ref[way] = out
        state = state.astype(BF16)
        for peer in range(send_ref.shape[0]):
            send_ref[peer, :, way * 2 * WIDE : (way + 1) * 2 * WIDE] = state


def advanced(piece, running):
    moved = dot(piece[:, WIDE:], by_head(running))
    if running.shape[1] == WIDE:
        return moved + piece[:, :WIDE]
    return moved + jnp.concatenate([piece[:, :WIDE], jnp.zeros((HEAD, WIDE), F32)], axis=1)


def combine_near(place_ref, got_ref, send_ref, pre_ref):
    y, z = place_ref[0], place_ref[1]
    start = jnp.concatenate([jnp.zeros((HEAD, WIDE), F32), head_eye()], axis=1)
    total, before = [start, start], [start, start]
    for step in range(8):
        for way in range(2):
            k = 7 - step if way else step
            piece = got_ref[k, :, way * 2 * WIDE : (way + 1) * 2 * WIDE].astype(F32)
            total[way] = advanced(piece, total[way])
            passed = (k > y) if way else (k < y)
            before[way] = jnp.where(passed, total[way], before[way])
    for way in range(2):
        pre_ref[way] = before[way]
    ahead, behind = total[0].astype(BF16), total[1].astype(BF16)
    for peer in range(8):
        send_ref[peer] = jnp.where(peer > z, ahead, behind)


def finish_mixer(
    place_ref,
    got_ref,
    pre_ref,
    local_ref,
    reads_ref,
    keys_ref,
    values_ref,
    rates_ref,
    valve_ref,
    reward_ref,
    gain_ref,
    projector_ref,
    send_ref,
):
    z = place_ref[1]
    state = [jnp.zeros((HEAD, WIDE), F32)] * 2
    for step in range(8):
        for way in range(2):
            k = 7 - step if way else step
            passed = (k > z) if way else (k < z)
            state[way] = jnp.where(
                passed, advanced(got_ref[k].astype(F32), state[way]), state[way]
            )
    summed = 0.0
    for way in range(2):
        entering = advanced(pre_ref[way], state[way])
        summed = summed + local_ref[way, :, :WIDE]
        summed = summed + dot(local_ref[way, :, WIDE:], by_head(entering))
    ones = head_ones()
    off = summed - dot(summed, ones) * (1.0 / HEAD)
    spread = dot(off * off, ones) * (1.0 / HEAD)
    normed = off * lax.rsqrt(spread + GROUP_EPS) * gain_ref[...]
    keys = keys_ref[...].astype(F32)
    both = keys * sigmoid(rates_ref[0].astype(F32)) + keys * sigmoid(rates_ref[1].astype(F32))
    bonus = dot(reads_ref[...].astype(F32) * both * reward_ref[...], ones)
    bonus = bonus * values_ref[...].astype(F32)
    mixed = ((normed + bonus) * valve_ref[...].astype(F32)).astype(BF16)
    share = jnp.dot(mixed, projector_ref[...], preferred_element_type=F32)
    send_ref[...] = share.astype(BF16).reshape(send_ref.shape)


def normed_rows(x, gain):
    off = x - jnp.mean(x, axis=-1, keepdims=True)
    spread = jnp.mean(off * off, axis=-1, keepdims=True)
    return off * lax.rsqrt(spread + NORM_EPS) * gain


def middle_rows(place_ref, got_ref, skip_ref, gain_ref, send_ref):
    summed = jnp.sum(got_ref[...].astype(F32), axis=0)
    summed = summed + RESIDUAL_SCALE * skip_ref[...].astype(F32)
    middle = normed_rows(summed, gain_ref[...]).astype(BF16)
    for peer in range(send_ref.shape[0]):
        send_ref[peer] = middle


def closing_rows(got_ref, middle_ref, gain_ref, out_ref):
    summed = jnp.sum(got_ref[...].astype(F32), axis=0)
    summed = summed + RESIDUAL_SCALE * middle_ref[0].astype(F32)
    out_ref[...] = normed_rows(summed, gain_ref[...]).astype(BF16)


def pack_weights(valve_ref, widen_ref, shrink_ref, send_ref):
    rows = valve_ref.shape[0]
    eye = (iota((rows, rows), 0) == iota((rows, rows), 1)).astype(BF16)
    turned = lax.dot_general(
        eye, shrink_ref[...], (((1,), (1,)), ((), ())), preferred_element_type=F32
    ).astype(BF16)
    blank = jnp.zeros((rows, 2 * PART - UNITS), BF16)
    halves = []
    for lo in (0, PART):
        line = []
        for whole in (valve_ref[...], widen_ref[...], turned):
            line.append(whole[:, lo : lo + PART])
            if lo:
                line.append(blank)
        halves.append(jnp.concatenate(line, axis=1))
    for peer in range(send_ref.shape[0]):
        send_ref[peer] = halves[peer % 2]


CHUNK = 1024
STEPS = D // CHUNK


def feed_forward(rows_ref, up_ref, down_ref, out_ref, acc_ref, inner_ref):
    step = pl.program_id(0)

    @pl.when(step < STEPS)
    def _():
        at = pl.multiple_of(step * CHUNK, CHUNK)
        part = jnp.dot(rows_ref[:, pl.ds(at, CHUNK)], up_ref[...], preferred_element_type=F32)
        acc_ref[...] = jnp.where(step == 0, part, acc_ref[...] + part)

    @pl.when(step == STEPS - 1)
    def _():
        gate, up = acc_ref[:, :PART], acc_ref[:, PART:]
        inner_ref[...] = (gate / (1.0 + jnp.exp(-gate)) * up).astype(BF16)

    @pl.when(step >= STEPS)
    def _():
        share = lax.dot_general(
            inner_ref[...], down_ref[...], (((1,), (1,)), ((), ())), preferred_element_type=F32
        )
        out_ref[...] = share.astype(BF16).reshape(out_ref.shape)


VMEM = pl.BlockSpec(memory_space=pltpu.VMEM)
SMEM = pl.BlockSpec(memory_space=pltpu.SMEM)


def shape(dims, kind=BF16):
    return jax.ShapeDtypeStruct(dims, kind)


def exchanged(value, axis):
    return lax.all_to_all(value, axis, 0, 0, tiled=True)


def run_mixer_local(*args):
    return pl.pallas_call(
        mixer_local,
        in_specs=[VMEM] * 6,
        out_specs=[VMEM] * 2,
        out_shape=[shape((8, HEAD, 4 * WIDE)), shape((2, TOK, 2 * WIDE), F32)],
        name="mixer_local",
    )(*args)


def run_combine_near(place, got):
    return pl.pallas_call(
        combine_near,
        in_specs=[SMEM, VMEM],
        out_specs=[VMEM] * 2,
        out_shape=[shape((8, HEAD, 2 * WIDE)), shape((2, HEAD, 2 * WIDE), F32)],
        name="combine_near",
    )(place, got)


def run_finish_mixer(place, *args):
    return pl.pallas_call(
        finish_mixer,
        in_specs=[SMEM] + [VMEM] * (len(args)),
        out_specs=VMEM,
        out_shape=shape((8, 8, D)),
        name="finish_mixer",
    )(place, *args)


def run_middle_rows(place, got, skip, gain, peers):
    return pl.pallas_call(
        middle_rows,
        grid_spec=pltpu.PrefetchScalarGridSpec(
            num_scalar_prefetch=1,
            grid=(1,),
            in_specs=[
                pl.BlockSpec((8, 8, D), lambda i, place: (0, 0, 0)),
                pl.BlockSpec((8, D), lambda i, place: (place[2], 0)),
                pl.BlockSpec((1, D), lambda i, place: (0, 0)),
            ],
            out_specs=pl.BlockSpec((peers, 8, D), lambda i, place: (0, 0, 0)),
        ),
        out_shape=shape((peers, 8, D)),
        name="middle_rows",
    )(place, got, skip, gain)


def run_feed_forward(rows, weights, peers):
    return pl.pallas_call(
        feed_forward,
        grid=(2 * STEPS,),
        in_specs=[
            pl.BlockSpec((peers * 8, D), lambda i: (0, 0)),
            pl.BlockSpec((CHUNK, 2 * PART), lambda i: (jnp.minimum(i, STEPS - 1), 0)),
            pl.BlockSpec((CHUNK, PART), lambda i: (jnp.maximum(i - STEPS, 0), 2)),
        ],
        out_specs=pl.BlockSpec((peers, 8, CHUNK), lambda i: (0, 0, jnp.maximum(i - STEPS, 0))),
        out_shape=shape((peers, 8, D)),
        scratch_shapes=[
            pltpu.VMEM((peers * 8, 2 * PART), F32),
            pltpu.VMEM((peers * 8, PART), BF16),
        ],
        name="feed_forward",
    )(rows, weights, weights)


def run_closing_rows(got, middle, gain):
    return pl.pallas_call(
        closing_rows,
        grid=(1,),
        in_specs=[
            pl.BlockSpec(got.shape, lambda i: (0, 0, 0)),
            pl.BlockSpec((1, 8, D), lambda i: (0, 0, 0)),
            pl.BlockSpec((1, D), lambda i: (0, 0)),
        ],
        out_specs=pl.BlockSpec((8, D), lambda i: (0, 0)),
        out_shape=shape((8, D)),
        name="closing_rows",
    )(got, middle, gain)


def shards(
    skip_stream_entering,
    reading_vectors,
    blender_lookup_labels,
    blender_payloads,
    blender_result_valve,
    fading_logits,
    amend_speed_logits,
    extra_log_fades,
    present_reward_factors,
    attender_scaling_vector,
    blender_result_projector,
    blender_scaling_vector,
    perceptron_valve_factors,
    perceptron_widen_factors,
    perceptron_shrink_factors,
    closing_scaling_vector,
):
    place = jnp.stack([lax.axis_index(Y), lax.axis_index("z"), lax.axis_index("tp")]).astype(
        jnp.int32
    )
    packed = pl.pallas_call(
        pack_weights,
        in_specs=[VMEM] * 3,
        out_specs=VMEM,
        out_shape=shape((8, 32, 3 * PART)),
        name="pack_weights",
    )(perceptron_valve_factors, perceptron_widen_factors, perceptron_shrink_factors)
    near_weights = exchanged(packed, Y).reshape(256, 3 * PART)
    weights = lax.all_gather(near_weights, "z", axis=0, tiled=True)

    sends, local = run_mixer_local(
        reading_vectors,
        blender_lookup_labels,
        blender_payloads,
        fading_logits,
        amend_speed_logits,
        extra_log_fades,
    )
    totals, before = run_combine_near(place, exchanged(sends, Y))
    shares = run_finish_mixer(
        place,
        exchanged(totals, "z"),
        before,
        local,
        reading_vectors,
        blender_lookup_labels,
        blender_payloads,
        amend_speed_logits,
        blender_result_valve,
        present_reward_factors.reshape(1, WIDE),
        attender_scaling_vector.reshape(1, WIDE),
        blender_result_projector,
    )
    peers = 16
    middle = run_middle_rows(
        place, exchanged(shares, "tp"), skip_stream_entering, blender_scaling_vector.reshape(1, D), peers
    )
    rows = exchanged(middle, PEERS).reshape(peers * 8, D)
    down = run_feed_forward(rows, weights, peers)
    return run_closing_rows(exchanged(down, PEERS), middle, closing_scaling_vector.reshape(1, D))


def solution(mesh):
    finer = Mesh(mesh.devices.reshape(8, 4, 2, mesh.shape["tp"]), SP_TP)
    placed = (
        P(SP, None),
        P(SP, "tp"),
        P(SP, "tp"),
        P(SP, "tp"),
        P(SP, "tp"),
        P(None, SP, "tp"),
        P(None, SP, "tp"),
        P(None, "tp", SP),
        P("tp"),
        P("tp"),
        P("tp", None),
        P(),
        P(SP, "tp"),
        P(SP, "tp"),
        P("tp", SP),
        P(),
    )
    return jax.shard_map(
        shards, mesh=finer, in_specs=placed, out_specs=P(SP_TP, None), check_vma=False
    )
```

```python
import math

import jax
import jax.numpy as jnp
from jax import lax
from jax.experimental import pallas as pl
from jax.experimental.pallas import tpu as pltpu
from jax.sharding import Mesh
from jax.sharding import PartitionSpec as P

Y = ("yh", "yl")
SP = ("z", "yh", "yl")
SP_TP = ("z", "yh", "yl", "tp")
PEERS = ("yl", "tp")

RESIDUAL_SCALE = 2.0**0.25
NORM_EPS = 1e-05
GROUP_EPS = 0.00064
KEY_EPS = 1e-06
TOK = 64
HEAD = 64
WIDE = 128
SUB = 16
UNITS = 704
PART = 384
D = 2048
F32 = jnp.float32
BF16 = jnp.bfloat16


def iota(shape, dim):
    return lax.broadcasted_iota(jnp.int32, shape, dim)


def dot(a, b):
    return jnp.dot(a, b, preferred_element_type=F32, precision=lax.Precision.HIGHEST)


def dot_nt(a, b):
    return lax.dot_general(
        a, b, (((1,), (1,)), ((), ())), preferred_element_type=F32, precision=lax.Precision.HIGHEST
    )


def dot_tn(a, b):
    return lax.dot_general(
        a, b, (((0,), (0,)), ((), ())), preferred_element_type=F32, precision=lax.Precision.HIGHEST
    )


def low_half(shape):
    return (iota(shape, len(shape) - 1) % WIDE) < HEAD


def by_head(x):
    low = low_half(x.shape)
    return jnp.concatenate([jnp.where(low, x, 0.0), jnp.where(low, 0.0, x)], axis=0)


def joined_heads(x):
    return x[:HEAD] + x[HEAD:]


def head_ones():
    return ((iota((WIDE, WIDE), 0) // HEAD) == (iota((WIDE, WIDE), 1) // HEAD)).astype(F32)


def head_eye():
    return (iota((HEAD, WIDE), 0) == iota((HEAD, WIDE), 1) % HEAD).astype(F32)


def sigmoid(x):
    return 1.0 / (1.0 + jnp.exp(-x))


def unit_lower_inverse(a):
    row, col = iota((WIDE, WIDE), 0), iota((WIDE, WIDE), 1)
    eye = (row == col).astype(F32)
    near = jnp.where(row // 8 == col // 8, a, 0.0)
    second = dot(near, near)
    fourth = dot(second, second)
    inverse = eye - near + second - dot(near, second)
    inverse = inverse + dot(inverse, fourth)
    for size in (8, 16, 32):
        across = (row // (2 * size) == col // (2 * size)) & (row // size != col // size)
        inverse = inverse - dot(inverse, dot(jnp.where(across, a, 0.0), inverse))
    return inverse


def one_way(back, reads, unit, keys, values, log_decay, rate):
    refill, write = unit * rate, keys * rate
    row, col = iota((TOK, TOK), 0), iota((TOK, TOK), 1)
    reach = (col >= row) if back else (col <= row)
    upto = dot(reach.astype(F32), log_decay)
    ahead = upto - log_decay
    whole = upto[:1] if back else upto[TOK - 1 :]
    low = low_half((SUB, WIDE))
    first, second = [], []
    for block in range(TOK // SUB):
        rows = slice(block * SUB, (block + 1) * SUB)
        edge = (block + 1) * SUB - 1 if back else block * SUB
        start = ahead[edge : edge + 1]
        scale = jnp.exp(jnp.minimum(start - upto, 60.0))
        erase_keys, write_keys = refill * scale, write * scale
        erased = unit[rows] * jnp.exp(ahead[rows] - start)
        read = reads[rows] * jnp.exp(upto[rows] - start)
        first.append(
            dot_nt(
                jnp.concatenate([jnp.where(low, erased, 0.0), jnp.where(low, read, 0.0)], axis=0),
                jnp.concatenate([erase_keys, write_keys], axis=0),
            )
        )
        second.append(
            dot_nt(
                jnp.concatenate([jnp.where(low, 0.0, erased), jnp.where(low, 0.0, read)], axis=0),
                jnp.concatenate([write_keys, erase_keys], axis=0),
            )
        )
    row, col = iota((TOK, WIDE), 0), iota((TOK, WIDE), 1) % HEAD
    past = (col > row) if back else (col < row)
    seen = (col >= row) if back else (col <= row)
    low = low_half((TOK, WIDE))

    def pieces(kept, lo):
        one = jnp.concatenate([part[lo : lo + SUB] for part in first], axis=0)
        two = jnp.concatenate([part[lo : lo + SUB] for part in second], axis=0)
        one, two = jnp.where(kept, one, 0.0), jnp.where(kept, two, 0.0)
        same = jnp.concatenate([jnp.where(low, one, 0.0), jnp.where(low, 0.0, two)], axis=0)
        other = jnp.concatenate([jnp.where(low, 0.0, one), jnp.where(low, two, 0.0)], axis=0)
        return same, other

    erase_erase, erase_write = pieces(past, 0)
    read_erase, read_write = pieces(seen, SUB)
    straight = by_head(values)
    crossed = jnp.concatenate([straight[TOK:], straight[:TOK]], axis=0)
    asked = jnp.concatenate([dot(erase_write, crossed), by_head(unit * jnp.exp(ahead))], axis=1)
    erased = -dot(unit_lower_inverse(erase_erase), asked)
    out = dot(read_erase, erased) + jnp.concatenate(
        [dot(read_write, crossed), by_head(reads * jnp.exp(upto))], axis=1
    )
    left = jnp.exp(whole - upto)
    state = dot_tn(by_head(refill * left), erased)
    state = joined_heads(state) + jnp.concatenate(
        [
            joined_heads(dot_tn(by_head(write * left), straight)),
            head_eye() * jnp.exp(whole),
        ],
        axis=1,
    )
    return joined_heads(out), state


def mixer_local(reads_ref, keys_ref, values_ref, fades_ref, rates_ref, extra_ref, send_ref, out_ref):
    reads, keys = reads_ref[...].astype(F32), keys_ref[...].astype(F32)
    values = values_ref[...].astype(F32)
    unit = keys * lax.rsqrt(dot(keys * keys, head_ones()) + KEY_EPS)
    lanes_of = (iota((2, WIDE), 1) // HEAD == iota((2, WIDE), 0)).astype(F32)
    for way in range(2):
        log_decay = -math.exp(-0.5) * sigmoid(fades_ref[way].astype(F32)) + dot_tn(
            extra_ref[way], lanes_of
        )
        rate = sigmoid(rates_ref[way].astype(F32))
        out, state = one_way(way == 1, reads, unit, keys, values, log_decay, rate)
        out_ref[way] = out
        state = state.astype(BF16)
        for peer in range(send_ref.shape[0]):
            send_ref[peer, :, way * 2 * WIDE : (way + 1) * 2 * WIDE] = state


def advanced(piece, running):
    moved = dot(piece[:, WIDE:], by_head(running))
    if running.shape[1] == WIDE:
        return moved + piece[:, :WIDE]
    return moved + jnp.concatenate([piece[:, :WIDE], jnp.zeros((HEAD, WIDE), F32)], axis=1)


def combine_near(place_ref, got_ref, send_ref, pre_ref):
    y, z = place_ref[0], place_ref[1]
    start = jnp.concatenate([jnp.zeros((HEAD, WIDE), F32), head_eye()], axis=1)
    total, before = [start, start], [start, start]
    for step in range(8):
        for way in range(2):
            k = 7 - step if way else step
            piece = got_ref[k, :, way * 2 * WIDE : (way + 1) * 2 * WIDE].astype(F32)
            total[way] = advanced(piece, total[way])
            passed = (k > y) if way else (k < y)
            before[way] = jnp.where(passed, total[way], before[way])
    for way in range(2):
        pre_ref[way] = before[way]
    ahead, behind = total[0].astype(BF16), total[1].astype(BF16)
    for peer in range(8):
        send_ref[peer] = jnp.where(peer > z, ahead, behind)


def finish_mixer(
    place_ref,
    got_ref,
    pre_ref,
    local_ref,
    reads_ref,
    keys_ref,
    values_ref,
    rates_ref,
    valve_ref,
    reward_ref,
    gain_ref,
    projector_ref,
    send_ref,
):
    z = place_ref[1]
    state = [jnp.zeros((HEAD, WIDE), F32)] * 2
    for step in range(8):
        for way in range(2):
            k = 7 - step if way else step
            passed = (k > z) if way else (k < z)
            state[way] = jnp.where(
                passed, advanced(got_ref[k].astype(F32), state[way]), state[way]
            )
    summed = 0.0
    for way in range(2):
        entering = advanced(pre_ref[way], state[way])
        summed = summed + local_ref[way, :, :WIDE]
        summed = summed + dot(local_ref[way, :, WIDE:], by_head(entering))
    ones = head_ones()
    off = summed - dot(summed, ones) * (1.0 / HEAD)
    spread = dot(off * off, ones) * (1.0 / HEAD)
    normed = off * lax.rsqrt(spread + GROUP_EPS) * gain_ref[...]
    keys = keys_ref[...].astype(F32)
    both = keys * sigmoid(rates_ref[0].astype(F32)) + keys * sigmoid(rates_ref[1].astype(F32))
    bonus = dot(reads_ref[...].astype(F32) * both * reward_ref[...], ones)
    bonus = bonus * values_ref[...].astype(F32)
    mixed = ((normed + bonus) * valve_ref[...].astype(F32)).astype(BF16)
    share = jnp.dot(mixed, projector_ref[...], preferred_element_type=F32)
    send_ref[...] = share.astype(BF16).reshape(send_ref.shape)


def normed_rows(x, gain):
    off = x - jnp.mean(x, axis=-1, keepdims=True)
    spread = jnp.mean(off * off, axis=-1, keepdims=True)
    return off * lax.rsqrt(spread + NORM_EPS) * gain


def middle_rows(place_ref, got_ref, skip_ref, gain_ref, send_ref):
    summed = jnp.sum(got_ref[...].astype(F32), axis=0)
    mine = skip_ref[pl.ds(pl.multiple_of(place_ref[2] * 8, 8), 8), :]
    summed = summed + RESIDUAL_SCALE * mine.astype(F32)
    middle = normed_rows(summed, gain_ref[...]).astype(BF16)
    for peer in range(send_ref.shape[0]):
        send_ref[peer] = middle


def closing_rows(got_ref, middle_ref, gain_ref, out_ref):
    summed = jnp.sum(got_ref[...].astype(F32), axis=0)
    summed = summed + RESIDUAL_SCALE * middle_ref[0].astype(F32)
    out_ref[...] = normed_rows(summed, gain_ref[...]).astype(BF16)


def pack_weights(valve_ref, widen_ref, shrink_ref, send_ref):
    blank = jnp.zeros((valve_ref.shape[0], 2 * PART - UNITS), BF16)
    halves = []
    for lo in (0, PART):
        line = []
        for whole in (valve_ref[...], widen_ref[...], shrink_ref[...]):
            line.append(whole[:, lo : lo + PART])
            if lo:
                line.append(blank)
        halves.append(jnp.concatenate(line, axis=1))
    for peer in range(send_ref.shape[0]):
        send_ref[peer] = halves[peer % 2]


CHUNK = 1024
STEPS = D // CHUNK


def feed_forward(rows_ref, up_ref, down_ref, out_ref, acc_ref, inner_ref):
    step = pl.program_id(0)

    @pl.when(step < STEPS)
    def _():
        at = pl.multiple_of(step * CHUNK, CHUNK)
        part = jnp.dot(rows_ref[:, pl.ds(at, CHUNK)], up_ref[...], preferred_element_type=F32)
        acc_ref[...] = jnp.where(step == 0, part, acc_ref[...] + part)

    @pl.when(step == STEPS - 1)
    def _():
        gate, up = acc_ref[:, :PART], acc_ref[:, PART:]
        inner_ref[...] = (gate / (1.0 + jnp.exp(-gate)) * up).astype(BF16)

    @pl.when(step >= STEPS)
    def _():
        share = lax.dot_general(
            inner_ref[...], down_ref[...], (((1,), (1,)), ((), ())), preferred_element_type=F32
        )
        out_ref[...] = share.astype(BF16).reshape(out_ref.shape)


VMEM = pl.BlockSpec(memory_space=pltpu.VMEM)
SMEM = pl.BlockSpec(memory_space=pltpu.SMEM)


def shape(dims, kind=BF16):
    return pltpu.VMEM(dims, kind)


def near(*arrays):
    return [pltpu.with_memory_space_constraint(a, pltpu.VMEM) for a in arrays]


def cost(us):
    return pl.CostEstimate(flops=int(us * 2.0e8), transcendentals=0, bytes_accessed=0)


def whole(array):
    return pl.BlockSpec(array.shape, lambda *_: (0,) * array.ndim)


def exchanged(value, axis):
    return lax.all_to_all(value, axis, 0, 0, tiled=True)


def run_mixer_local(*args):
    return pl.pallas_call(
        mixer_local,
        grid=(1,),
        in_specs=[whole(a) for a in args],
        out_specs=[VMEM] * 2,
        out_shape=[shape((8, HEAD, 4 * WIDE)), shape((2, TOK, 2 * WIDE), F32)],
        cost_estimate=cost(8),
        name="mixer_local",
    )(*args)


def run_combine_near(place, got):
    return pl.pallas_call(
        combine_near,
        in_specs=[SMEM, VMEM],
        out_specs=[VMEM] * 2,
        out_shape=[shape((8, HEAD, 2 * WIDE)), shape((2, HEAD, 2 * WIDE), F32)],
        cost_estimate=cost(3),
        name="combine_near",
    )(place, *near(got))


def run_finish_mixer(place, *args):
    return pl.pallas_call(
        finish_mixer,
        in_specs=[SMEM] + [VMEM] * (len(args)),
        out_specs=VMEM,
        out_shape=shape((8, 8, D)),
        cost_estimate=cost(4),
        name="finish_mixer",
    )(place, *near(*args))


def run_middle_rows(place, got, skip, gain, peers):
    return pl.pallas_call(
        middle_rows,
        in_specs=[SMEM] + [VMEM] * 3,
        out_specs=VMEM,
        out_shape=shape((peers, 8, D)),
        cost_estimate=cost(2),
        name="middle_rows",
    )(place, *near(got, skip, gain))


def run_feed_forward(rows, weights, peers):
    return pl.pallas_call(
        feed_forward,
        grid=(2 * STEPS,),
        in_specs=[
            pl.BlockSpec((peers * 8, D), lambda i: (0, 0)),
            pl.BlockSpec((CHUNK, 2 * PART), lambda i: (jnp.minimum(i, STEPS - 1), 0)),
            pl.BlockSpec((CHUNK, PART), lambda i: (jnp.maximum(i - STEPS, 0), 2)),
        ],
        out_specs=pl.BlockSpec((peers, 8, CHUNK), lambda i: (0, 0, jnp.maximum(i - STEPS, 0))),
        out_shape=shape((peers, 8, D)),
        scratch_shapes=[
            pltpu.VMEM((peers * 8, 2 * PART), F32),
            pltpu.VMEM((peers * 8, PART), BF16),
        ],
        cost_estimate=cost(5),
        name="feed_forward",
    )(*near(rows), weights, weights)


def run_closing_rows(got, middle, gain):
    return pl.pallas_call(
        closing_rows,
        in_specs=[VMEM] * 3,
        out_specs=VMEM,
        out_shape=jax.ShapeDtypeStruct((8, D), BF16),
        cost_estimate=cost(2),
        name="closing_rows",
    )(*near(got, middle, gain))


def shards(
    skip_stream_entering,
    reading_vectors,
    blender_lookup_labels,
    blender_payloads,
    blender_result_valve,
    fading_logits,
    amend_speed_logits,
    extra_log_fades,
    present_reward_factors,
    attender_scaling_vector,
    blender_result_projector,
    blender_scaling_vector,
    perceptron_valve_factors,
    perceptron_widen_factors,
    perceptron_shrink_factors,
    closing_scaling_vector,
):
    place = jnp.stack([lax.axis_index(Y), lax.axis_index("z"), lax.axis_index("tp")]).astype(
        jnp.int32
    )
    given = (perceptron_valve_factors, perceptron_widen_factors, perceptron_shrink_factors.T)
    packed = pl.pallas_call(
        pack_weights,
        grid=(1,),
        in_specs=[whole(a) for a in given],
        out_specs=VMEM,
        out_shape=shape((8, 32, 3 * PART)),
        cost_estimate=cost(2),
        name="pack_weights",
    )(*given)
    near_weights = exchanged(packed, Y)
    sends, local = run_mixer_local(
        reading_vectors,
        blender_lookup_labels,
        blender_payloads,
        fading_logits,
        amend_speed_logits,
        extra_log_fades,
    )
    weights = lax.all_gather(near_weights.reshape(256, 3 * PART), "z", axis=0, tiled=True)
    totals, before = run_combine_near(place, exchanged(sends, Y))
    shares = run_finish_mixer(
        place,
        exchanged(totals, "z"),
        before,
        local,
        reading_vectors,
        blender_lookup_labels,
        blender_payloads,
        amend_speed_logits,
        blender_result_valve,
        present_reward_factors.reshape(1, WIDE),
        attender_scaling_vector.reshape(1, WIDE),
        blender_result_projector,
    )
    peers = 16
    middle = run_middle_rows(
        place, exchanged(shares, "tp"), skip_stream_entering, blender_scaling_vector.reshape(1, D), peers
    )
    rows = exchanged(middle, PEERS).reshape(peers * 8, D)
    down = run_feed_forward(rows, weights, peers)
    return run_closing_rows(exchanged(down, PEERS), middle, closing_scaling_vector.reshape(1, D))


def solution(mesh):
    finer = Mesh(mesh.devices.reshape(8, 4, 2, mesh.shape["tp"]), SP_TP)
    placed = (
        P(SP, None),
        P(SP, "tp"),
        P(SP, "tp"),
        P(SP, "tp"),
        P(SP, "tp"),
        P(None, SP, "tp"),
        P(None, SP, "tp"),
        P(None, "tp", SP),
        P("tp"),
        P("tp"),
        P("tp", None),
        P(),
        P(SP, "tp"),
        P(SP, "tp"),
        P("tp", SP),
        P(),
    )
    return jax.shard_map(
        shards, mesh=finer, in_specs=placed, out_specs=P(SP_TP, None), check_vma=False
    )
```

```python
import math

import jax
import jax.numpy as jnp
from jax import lax
from jax.experimental import pallas as pl
from jax.experimental.pallas import tpu as pltpu
from jax.sharding import Mesh
from jax.sharding import PartitionSpec as P

Y = ("yh", "yl")
SP = ("z", "yh", "yl")
SP_TP = SP + ("tp",)
PEERS = ("yl", "tp")

RESIDUAL_SCALE = 2.0**0.25
NORM_EPS = 1e-05
GROUP_EPS = 0.00064
KEY_EPS = 1e-06
TOK = 64
HEAD = 64
WIDE = 128
SUB = 16
UNITS = 704
PART = 384
PEER_COUNT = 16
D = 2048
F32 = jnp.float32
BF16 = jnp.bfloat16


def iota(shape, dim):
    return lax.broadcasted_iota(jnp.int32, shape, dim)


def split(x):
    high = x.astype(BF16)
    return high, (x - high.astype(F32)).astype(BF16)


def product(a, b, dims):
    (a_high, a_low), (b_high, b_low) = split(a), split(b)

    def part(one, two):
        return lax.dot_general(one, two, (dims, ((), ())), preferred_element_type=F32)

    return part(a_high, b_high) + (part(a_high, b_low) + part(a_low, b_high))


def dot(a, b):
    return product(a, b, ((1,), (0,)))


def dot_nt(a, b):
    return product(a, b, ((1,), (1,)))


def dot_tn(a, b):
    return product(a, b, ((0,), (0,)))


def chosen(picks, x, dims=((1,), (0,))):
    high, middle = split(x)
    low = (x - high.astype(F32) - middle.astype(F32)).astype(BF16)
    parts = [
        lax.dot_general(picks, part, (dims, ((), ())), preferred_element_type=F32)
        for part in (high, middle, low)
    ]
    return parts[0] + (parts[1] + parts[2])


def head_sums(x):
    high, low = split(x)
    ones = head_ones().astype(BF16)
    return jnp.dot(high, ones, preferred_element_type=F32) + jnp.dot(
        low, ones, preferred_element_type=F32
    )


def low_half(shape):
    return (iota(shape, len(shape) - 1) % WIDE) < HEAD


def by_head(x):
    low = low_half(x.shape)
    return jnp.concatenate([jnp.where(low, x, 0.0), jnp.where(low, 0.0, x)], axis=0)


def joined_heads(x):
    return x[:HEAD] + x[HEAD:]


def head_ones():
    return ((iota((WIDE, WIDE), 0) // HEAD) == (iota((WIDE, WIDE), 1) // HEAD)).astype(F32)


def head_eye():
    return (iota((HEAD, WIDE), 0) == iota((HEAD, WIDE), 1) % HEAD).astype(F32)


def sigmoid(x):
    return 1.0 / (1.0 + jnp.exp(-x))


def spread_heads(extra):
    lanes_of = (iota((2, WIDE), 1) // HEAD == iota((2, WIDE), 0)).astype(BF16)
    high, middle = split(extra)
    low = (extra - high.astype(F32) - middle.astype(F32)).astype(BF16)
    parts = [
        lax.dot_general(part, lanes_of, (((0,), (0,)), ((), ())), preferred_element_type=F32)
        for part in (high, middle, low)
    ]
    return parts[0] + (parts[1] + parts[2])


def unit_lower_inverse(a):
    row, col = iota((WIDE, WIDE), 0), iota((WIDE, WIDE), 1)
    eye = (row == col).astype(F32)
    near = jnp.where(row // 8 == col // 8, a, 0.0)
    second = dot(near, near)
    fourth = dot(second, second)
    inverse = eye - near + second - dot(near, second)
    inverse = inverse + dot(inverse, fourth)
    for size in (8, 16, 32):
        across = (row // (2 * size) == col // (2 * size)) & (row // size != col // size)
        inverse = inverse - dot(inverse, dot(jnp.where(across, a, 0.0), inverse))
    return inverse


def one_way(back, reads, unit, keys, values, log_decay, rate):
    refill, write = unit * rate, keys * rate
    row, col = iota((TOK, TOK), 0), iota((TOK, TOK), 1)
    reach = (col >= row) if back else (col <= row)
    upto = chosen(reach.astype(BF16), log_decay)
    ahead = upto - log_decay
    whole = upto[:1] if back else upto[TOK - 1 :]
    low = low_half((SUB, WIDE))
    first, second = [], []
    for block in range(TOK // SUB):
        rows = slice(block * SUB, (block + 1) * SUB)
        edge = (block + 1) * SUB - 1 if back else block * SUB
        start = ahead[edge : edge + 1]
        scale = jnp.exp(jnp.minimum(start - upto, 60.0))
        erase_keys, write_keys = refill * scale, write * scale
        erased = unit[rows] * jnp.exp(ahead[rows] - start)
        read = reads[rows] * jnp.exp(upto[rows] - start)
        first.append(
            dot_nt(
                jnp.concatenate([jnp.where(low, erased, 0.0), jnp.where(low, read, 0.0)], axis=0),
                jnp.concatenate([erase_keys, write_keys], axis=0),
            )
        )
        second.append(
            dot_nt(
                jnp.concatenate([jnp.where(low, 0.0, erased), jnp.where(low, 0.0, read)], axis=0),
                jnp.concatenate([write_keys, erase_keys], axis=0),
            )
        )
    row, col = iota((TOK, WIDE), 0), iota((TOK, WIDE), 1) % HEAD
    past = (col > row) if back else (col < row)
    seen = (col >= row) if back else (col <= row)
    low = low_half((TOK, WIDE))

    def pieces(kept, lo):
        one = jnp.concatenate([part[lo : lo + SUB] for part in first], axis=0)
        two = jnp.concatenate([part[lo : lo + SUB] for part in second], axis=0)
        one, two = jnp.where(kept, one, 0.0), jnp.where(kept, two, 0.0)
        same = jnp.concatenate([jnp.where(low, one, 0.0), jnp.where(low, 0.0, two)], axis=0)
        other = jnp.concatenate([jnp.where(low, 0.0, one), jnp.where(low, two, 0.0)], axis=0)
        return same, other

    erase_erase, erase_write = pieces(past, 0)
    read_erase, read_write = pieces(seen, SUB)
    straight = by_head(values)
    crossed = jnp.concatenate([straight[TOK:], straight[:TOK]], axis=0)
    asked = jnp.concatenate([dot(erase_write, crossed), by_head(unit * jnp.exp(ahead))], axis=1)
    erased = -dot(unit_lower_inverse(erase_erase), asked)
    out = dot(read_erase, erased) + jnp.concatenate(
        [dot(read_write, crossed), by_head(reads * jnp.exp(upto))], axis=1
    )
    left = jnp.exp(whole - upto)
    state = dot_tn(by_head(refill * left), erased)
    state = joined_heads(state) + jnp.concatenate(
        [
            joined_heads(dot_tn(by_head(write * left), straight)),
            head_eye() * jnp.exp(whole),
        ],
        axis=1,
    )
    return joined_heads(out), state


def mixer_local(reads_ref, keys_ref, values_ref, fades_ref, rates_ref, extra_ref, send_ref, out_ref):
    reads, keys = reads_ref[...].astype(F32), keys_ref[...].astype(F32)
    values = values_ref[...].astype(F32)
    unit = keys * lax.rsqrt(head_sums(keys * keys) + KEY_EPS)
    for way in range(2):
        log_decay = -math.exp(-0.5) * sigmoid(fades_ref[way].astype(F32))
        log_decay = log_decay + spread_heads(extra_ref[way])
        rate = sigmoid(rates_ref[way].astype(F32))
        out, state = one_way(way == 1, reads, unit, keys, values, log_decay, rate)
        out_ref[way] = out
        state = state.astype(BF16)
        for peer in range(send_ref.shape[0]):
            send_ref[peer, :, way * 2 * WIDE : (way + 1) * 2 * WIDE] = state


def advanced(piece, running):
    high, low = split(by_head(running))
    step = piece[:, WIDE:]
    if step.dtype == F32:
        moved = dot(step, by_head(running))
    else:
        moved = jnp.dot(step, high, preferred_element_type=F32)
        moved = moved + jnp.dot(step, low, preferred_element_type=F32)
    if running.shape[1] == WIDE:
        return moved + piece[:, :WIDE]
    return moved + jnp.concatenate([piece[:, :WIDE], jnp.zeros((HEAD, WIDE), F32)], axis=1)


def combine_near(place_ref, got_ref, send_ref, pre_ref):
    y, z = place_ref[0], place_ref[1]
    start = jnp.concatenate([jnp.zeros((HEAD, WIDE), F32), head_eye()], axis=1)
    total, before = [start, start], [start, start]
    for step in range(8):
        for way in range(2):
            k = 7 - step if way else step
            piece = got_ref[k, :, way * 2 * WIDE : (way + 1) * 2 * WIDE]
            total[way] = advanced(piece, total[way])
            passed = (k > y) if way else (k < y)
            before[way] = jnp.where(passed, total[way], before[way])
    for way in range(2):
        pre_ref[way] = before[way]
    ahead, behind = total[0].astype(BF16), total[1].astype(BF16)
    for peer in range(8):
        send_ref[peer] = jnp.where(peer > z, ahead, behind)


def finish_mixer(
    place_ref,
    got_ref,
    pre_ref,
    local_ref,
    reads_ref,
    keys_ref,
    values_ref,
    rates_ref,
    valve_ref,
    reward_ref,
    gain_ref,
    projector_ref,
    send_ref,
):
    z = place_ref[1]
    state = [jnp.zeros((HEAD, WIDE), F32)] * 2
    for step in range(8):
        for way in range(2):
            k = 7 - step if way else step
            passed = (k > z) if way else (k < z)
            state[way] = jnp.where(
                passed, advanced(got_ref[k], state[way]), state[way]
            )
    summed = 0.0
    for way in range(2):
        entering = advanced(pre_ref[way], state[way])
        summed = summed + local_ref[way, :, :WIDE]
        summed = summed + dot(local_ref[way, :, WIDE:], by_head(entering))
    off = summed - head_sums(summed) * (1.0 / HEAD)
    spread = head_sums(off * off) * (1.0 / HEAD)
    normed = off * lax.rsqrt(spread + GROUP_EPS) * gain_ref[...]
    keys = keys_ref[...].astype(F32)
    both = keys * sigmoid(rates_ref[0].astype(F32)) + keys * sigmoid(rates_ref[1].astype(F32))
    bonus = head_sums(reads_ref[...].astype(F32) * both * reward_ref[...])
    bonus = bonus * values_ref[...].astype(F32)
    mixed = ((normed + bonus) * valve_ref[...].astype(F32)).astype(BF16)
    share = jnp.dot(mixed, projector_ref[...], preferred_element_type=F32)
    send_ref[...] = share.astype(BF16).reshape(send_ref.shape)


def normed_rows(x, gain):
    off = x - jnp.mean(x, axis=-1, keepdims=True)
    spread = jnp.mean(off * off, axis=-1, keepdims=True)
    return off * lax.rsqrt(spread + NORM_EPS) * gain


def middle_rows(place_ref, got_ref, skip_ref, gain_ref, send_ref):
    summed = jnp.sum(got_ref[...].astype(F32), axis=0)
    mine = skip_ref[pl.ds(pl.multiple_of(place_ref[2] * 8, 8), 8), :]
    summed = summed + RESIDUAL_SCALE * mine.astype(F32)
    middle = normed_rows(summed, gain_ref[...]).astype(BF16)
    for peer in range(send_ref.shape[0]):
        send_ref[peer] = middle


def closing_rows(got_ref, middle_ref, gain_ref, out_ref):
    summed = jnp.sum(got_ref[...].astype(F32), axis=0)
    summed = summed + RESIDUAL_SCALE * middle_ref[0].astype(F32)
    out_ref[...] = normed_rows(summed, gain_ref[...]).astype(BF16)


def pack_weights(valve_ref, widen_ref, shrink_ref, send_ref):
    blank = jnp.zeros((valve_ref.shape[0], 2 * PART - UNITS), BF16)
    halves = []
    for lo in (0, PART):
        line = []
        for whole in (valve_ref[...], widen_ref[...], shrink_ref[...]):
            line.append(whole[:, lo : lo + PART])
            if lo:
                line.append(blank)
        halves.append(jnp.concatenate(line, axis=1))
    for peer in range(send_ref.shape[0]):
        send_ref[peer] = halves[peer % 2]


PLANE = 256
PARTS = D // PLANE


def feed_forward(rows_ref, weights_ref, out_ref, held_ref, arrived):
    copies = []
    for k in range(PARTS):
        rows = pl.ds(k * PLANE, PLANE)
        copies.append(
            pltpu.make_async_copy(weights_ref.at[rows], held_ref.at[rows], arrived.at[k])
        )
        copies[k].start()
    sums = 0.0
    for k in range(PARTS):
        copies[k].wait()
        rows = slice(k * PLANE, (k + 1) * PLANE)
        sums = sums + jnp.dot(
            rows_ref[:, rows], held_ref[rows, : 2 * PART], preferred_element_type=F32
        )
    gate, up = sums[:, :PART], sums[:, PART:]
    inner = (gate / (1.0 + jnp.exp(-gate)) * up).astype(BF16)
    for k in range(PARTS):
        rows = slice(k * PLANE, (k + 1) * PLANE)
        share = lax.dot_general(
            inner, held_ref[rows, 2 * PART :], (((1,), (1,)), ((), ())), preferred_element_type=F32
        )
        out_ref[:, :, rows] = share.astype(BF16).reshape(PEER_COUNT, 8, PLANE)


VMEM = pl.BlockSpec(memory_space=pltpu.VMEM)
SMEM = pl.BlockSpec(memory_space=pltpu.SMEM)


def shape(dims, kind=BF16):
    return pltpu.VMEM(dims, kind)


def near(*arrays):
    return [pltpu.with_memory_space_constraint(a, pltpu.VMEM) for a in arrays]


def cost(us):
    return pl.CostEstimate(flops=int(us * 2.0e8), transcendentals=0, bytes_accessed=0)


def whole(array):
    return pl.BlockSpec(array.shape, lambda *_: (0,) * array.ndim)


def exchanged(value, axis):
    return lax.all_to_all(value, axis, 0, 0, tiled=True)


def run_mixer_local(*args):
    return pl.pallas_call(
        mixer_local,
        grid=(1,),
        in_specs=[whole(a) for a in args],
        out_specs=[VMEM] * 2,
        out_shape=[shape((8, HEAD, 4 * WIDE)), shape((2, TOK, 2 * WIDE), F32)],
        cost_estimate=cost(8),
        name="mixer_local",
    )(*args)


def run_combine_near(place, got):
    return pl.pallas_call(
        combine_near,
        in_specs=[SMEM, VMEM],
        out_specs=[VMEM] * 2,
        out_shape=[shape((8, HEAD, 2 * WIDE)), shape((2, HEAD, 2 * WIDE), F32)],
        cost_estimate=cost(3),
        name="combine_near",
    )(place, *near(got))


def run_finish_mixer(place, *args):
    return pl.pallas_call(
        finish_mixer,
        in_specs=[SMEM] + [VMEM] * (len(args)),
        out_specs=VMEM,
        out_shape=shape((8, 8, D)),
        cost_estimate=cost(4),
        name="finish_mixer",
    )(place, *near(*args))


def run_middle_rows(place, got, skip, gain, peers):
    return pl.pallas_call(
        middle_rows,
        in_specs=[SMEM] + [VMEM] * 3,
        out_specs=VMEM,
        out_shape=shape((peers, 8, D)),
        cost_estimate=cost(2),
        name="middle_rows",
    )(place, *near(got, skip, gain))


def run_feed_forward(rows, weights):
    return pl.pallas_call(
        feed_forward,
        in_specs=[VMEM, pl.BlockSpec(memory_space=pl.ANY)],
        out_specs=VMEM,
        out_shape=shape((PEER_COUNT, 8, D)),
        scratch_shapes=[
            pltpu.VMEM((D, 3 * PART), BF16),
            pltpu.SemaphoreType.DMA((PARTS,)),
        ],
        cost_estimate=cost(4),
        name="feed_forward",
    )(*near(rows), weights)


def run_closing_rows(got, middle, gain):
    return pl.pallas_call(
        closing_rows,
        in_specs=[VMEM] * 3,
        out_specs=VMEM,
        out_shape=jax.ShapeDtypeStruct((8, D), BF16),
        cost_estimate=cost(2),
        name="closing_rows",
    )(*near(got, middle, gain))


def shards(
    skip_stream_entering,
    reading_vectors,
    blender_lookup_labels,
    blender_payloads,
    blender_result_valve,
    fading_logits,
    amend_speed_logits,
    extra_log_fades,
    present_reward_factors,
    attender_scaling_vector,
    blender_result_projector,
    blender_scaling_vector,
    perceptron_valve_factors,
    perceptron_widen_factors,
    perceptron_shrink_factors,
    closing_scaling_vector,
):
    place = jnp.stack([lax.axis_index(Y), lax.axis_index("z"), lax.axis_index("tp")]).astype(
        jnp.int32
    )
    given = (perceptron_valve_factors, perceptron_widen_factors, perceptron_shrink_factors.T)
    packed = pl.pallas_call(
        pack_weights,
        grid=(1,),
        in_specs=[whole(a) for a in given],
        out_specs=VMEM,
        out_shape=shape((8, 32, 3 * PART)),
        cost_estimate=cost(2),
        name="pack_weights",
    )(*given)
    own = exchanged(packed, Y).reshape(PLANE, 3 * PART)
    sends, local = run_mixer_local(
        reading_vectors,
        blender_lookup_labels,
        blender_payloads,
        fading_logits,
        amend_speed_logits,
        extra_log_fades,
    )
    near_states = exchanged(sends, Y)
    weights = [lax.all_gather(own, "z", axis=0, tiled=True)]
    totals, before = run_combine_near(place, near_states)
    far_states = exchanged(totals, "z")
    shares = run_finish_mixer(
        place,
        far_states,
        before,
        local,
        reading_vectors,
        blender_lookup_labels,
        blender_payloads,
        amend_speed_logits,
        blender_result_valve,
        present_reward_factors.reshape(1, WIDE),
        attender_scaling_vector.reshape(1, WIDE),
        blender_result_projector,
    )
    shares = exchanged(shares, "tp")
    middle = run_middle_rows(
        place, shares, skip_stream_entering, blender_scaling_vector.reshape(1, D), PEER_COUNT
    )
    rows = exchanged(middle, PEERS).reshape(PEER_COUNT * 8, D)
    down = run_feed_forward(rows, weights[0])
    down = exchanged(down, PEERS)
    return run_closing_rows(down, middle, closing_scaling_vector.reshape(1, D))


def solution(mesh):
    finer = Mesh(mesh.devices.reshape(8, 4, 2, mesh.shape["tp"]), SP_TP)
    placed = (
        P(SP, None),
        P(SP, "tp"),
        P(SP, "tp"),
        P(SP, "tp"),
        P(SP, "tp"),
        P(None, SP, "tp"),
        P(None, SP, "tp"),
        P(None, "tp", SP),
        P("tp"),
        P("tp"),
        P("tp", None),
        P(),
        P(SP, "tp"),
        P(SP, "tp"),
        P("tp", SP),
        P(),
    )
    return jax.shard_map(
        shards, mesh=finer, in_specs=placed, out_specs=P(SP_TP, None), check_vma=False
    )
```

```python
import math

import jax
import jax.numpy as jnp
from jax import lax
from jax.experimental import pallas as pl
from jax.experimental.pallas import tpu as pltpu
from jax.sharding import Mesh
from jax.sharding import PartitionSpec as P

Y = ("yh", "yl")
SP = ("z", "yh", "yl")
SP_TP = SP + ("tp",)
PEERS = ("yl", "tp")

RESIDUAL_SCALE = 2.0**0.25
NORM_EPS = 1e-05
GROUP_EPS = 0.00064
KEY_EPS = 1e-06
TOK = 64
HEAD = 64
WIDE = 128
SUB = 16
UNITS = 704
PART = 384
PEER_COUNT = 16
D = 2048
F32 = jnp.float32
BF16 = jnp.bfloat16


def iota(shape, dim):
    return lax.broadcasted_iota(jnp.int32, shape, dim)


def split(x):
    high = x.astype(BF16)
    return high, (x - high.astype(F32)).astype(BF16)


def product(a, b, dims):
    (a_high, a_low), (b_high, b_low) = split(a), split(b)

    def part(one, two):
        return lax.dot_general(one, two, (dims, ((), ())), preferred_element_type=F32)

    return part(a_high, b_high) + (part(a_high, b_low) + part(a_low, b_high))


def dot(a, b):
    return product(a, b, ((1,), (0,)))


def dot_nt(a, b):
    return product(a, b, ((1,), (1,)))


def dot_tn(a, b):
    return product(a, b, ((0,), (0,)))


def chosen(picks, x, dims=((1,), (0,))):
    high, middle = split(x)
    low = (x - high.astype(F32) - middle.astype(F32)).astype(BF16)
    parts = [
        lax.dot_general(picks, part, (dims, ((), ())), preferred_element_type=F32)
        for part in (high, middle, low)
    ]
    return parts[0] + (parts[1] + parts[2])


def head_sums(x):
    high, low = split(x)
    ones = head_ones().astype(BF16)
    return jnp.dot(high, ones, preferred_element_type=F32) + jnp.dot(
        low, ones, preferred_element_type=F32
    )


def low_half(shape):
    return (iota(shape, len(shape) - 1) % WIDE) < HEAD


def by_head(x):
    low = low_half(x.shape)
    return jnp.concatenate([jnp.where(low, x, 0.0), jnp.where(low, 0.0, x)], axis=0)


def joined_heads(x):
    return x[:HEAD] + x[HEAD:]


def head_ones():
    return ((iota((WIDE, WIDE), 0) // HEAD) == (iota((WIDE, WIDE), 1) // HEAD)).astype(F32)


def head_eye():
    return (iota((HEAD, WIDE), 0) == iota((HEAD, WIDE), 1) % HEAD).astype(F32)


def sigmoid(x):
    return 1.0 / (1.0 + jnp.exp(-x))


def spread_heads(extra):
    lanes_of = (iota((2, WIDE), 1) // HEAD == iota((2, WIDE), 0)).astype(BF16)
    high, middle = split(extra)
    low = (extra - high.astype(F32) - middle.astype(F32)).astype(BF16)
    parts = [
        lax.dot_general(part, lanes_of, (((0,), (0,)), ((), ())), preferred_element_type=F32)
        for part in (high, middle, low)
    ]
    return parts[0] + (parts[1] + parts[2])


def unit_lower_inverse(a):
    row, col = iota((WIDE, WIDE), 0), iota((WIDE, WIDE), 1)
    eye = (row == col).astype(F32)
    near = jnp.where(row // 8 == col // 8, a, 0.0)
    second = dot(near, near)
    fourth = dot(second, second)
    inverse = eye - near + second - dot(near, second)
    inverse = inverse + dot(inverse, fourth)
    for size in (8, 16, 32):
        across = (row // (2 * size) == col // (2 * size)) & (row // size != col // size)
        inverse = inverse - dot(inverse, dot(jnp.where(across, a, 0.0), inverse))
    return inverse


def one_way(back, reads, unit, keys, values, log_decay, rate):
    refill, write = unit * rate, keys * rate
    row, col = iota((TOK, TOK), 0), iota((TOK, TOK), 1)
    reach = (col >= row) if back else (col <= row)
    upto = chosen(reach.astype(BF16), log_decay)
    ahead = upto - log_decay
    whole = upto[:1] if back else upto[TOK - 1 :]
    low = low_half((SUB, WIDE))
    first, second = [], []
    for block in range(TOK // SUB):
        rows = slice(block * SUB, (block + 1) * SUB)
        edge = (block + 1) * SUB - 1 if back else block * SUB
        start = ahead[edge : edge + 1]
        scale = jnp.exp(jnp.minimum(start - upto, 60.0))
        erase_keys, write_keys = refill * scale, write * scale
        erased = unit[rows] * jnp.exp(ahead[rows] - start)
        read = reads[rows] * jnp.exp(upto[rows] - start)
        first.append(
            dot_nt(
                jnp.concatenate([jnp.where(low, erased, 0.0), jnp.where(low, read, 0.0)], axis=0),
                jnp.concatenate([erase_keys, write_keys], axis=0),
            )
        )
        second.append(
            dot_nt(
                jnp.concatenate([jnp.where(low, 0.0, erased), jnp.where(low, 0.0, read)], axis=0),
                jnp.concatenate([write_keys, erase_keys], axis=0),
            )
        )
    row, col = iota((TOK, WIDE), 0), iota((TOK, WIDE), 1) % HEAD
    past = (col > row) if back else (col < row)
    seen = (col >= row) if back else (col <= row)
    low = low_half((TOK, WIDE))

    def pieces(kept, lo):
        one = jnp.concatenate([part[lo : lo + SUB] for part in first], axis=0)
        two = jnp.concatenate([part[lo : lo + SUB] for part in second], axis=0)
        one, two = jnp.where(kept, one, 0.0), jnp.where(kept, two, 0.0)
        same = jnp.concatenate([jnp.where(low, one, 0.0), jnp.where(low, 0.0, two)], axis=0)
        other = jnp.concatenate([jnp.where(low, 0.0, one), jnp.where(low, two, 0.0)], axis=0)
        return same, other

    erase_erase, erase_write = pieces(past, 0)
    read_erase, read_write = pieces(seen, SUB)
    straight = by_head(values)
    crossed = jnp.concatenate([straight[TOK:], straight[:TOK]], axis=0)
    asked = jnp.concatenate([dot(erase_write, crossed), by_head(unit * jnp.exp(ahead))], axis=1)
    erased = -dot(unit_lower_inverse(erase_erase), asked)
    out = dot(read_erase, erased) + jnp.concatenate(
        [dot(read_write, crossed), by_head(reads * jnp.exp(upto))], axis=1
    )
    left = jnp.exp(whole - upto)
    state = dot_tn(by_head(refill * left), erased)
    state = joined_heads(state) + jnp.concatenate(
        [
            joined_heads(dot_tn(by_head(write * left), straight)),
            head_eye() * jnp.exp(whole),
        ],
        axis=1,
    )
    return joined_heads(out), state


def mixer_local(place_ref, reads_ref, keys_ref, values_ref, fades_ref, rates_ref, extra_ref, send_ref, out_ref):
    reads, keys = reads_ref[...].astype(F32), keys_ref[...].astype(F32)
    values = values_ref[...].astype(F32)
    unit = keys * lax.rsqrt(head_sums(keys * keys) + KEY_EPS)
    for way in range(2):
        log_decay = -math.exp(-0.5) * sigmoid(fades_ref[way].astype(F32))
        log_decay = log_decay + spread_heads(extra_ref[way])
        rate = sigmoid(rates_ref[way].astype(F32))
        out, state = one_way(way == 1, reads, unit, keys, values, log_decay, rate)
        out_ref[way] = out
        state = state.astype(BF16)
        for peer in range(send_ref.shape[0]):
            send_ref[peer, :, way * 2 * WIDE : (way + 1) * 2 * WIDE] = state


def advanced(piece, running):
    high, low = split(by_head(running))
    step = piece[:, WIDE:]
    if step.dtype == F32:
        moved = dot(step, by_head(running))
    else:
        moved = jnp.dot(step, high, preferred_element_type=F32)
        moved = moved + jnp.dot(step, low, preferred_element_type=F32)
    if running.shape[1] == WIDE:
        return moved + piece[:, :WIDE]
    return moved + jnp.concatenate([piece[:, :WIDE], jnp.zeros((HEAD, WIDE), F32)], axis=1)


def combine_near(place_ref, got_ref, send_ref, pre_ref):
    y, z = place_ref[0], place_ref[1]
    start = jnp.concatenate([jnp.zeros((HEAD, WIDE), F32), head_eye()], axis=1)
    total, before = [start, start], [start, start]
    for step in range(8):
        for way in range(2):
            k = 7 - step if way else step
            piece = got_ref[k, :, way * 2 * WIDE : (way + 1) * 2 * WIDE]
            total[way] = advanced(piece, total[way]) if step else piece.astype(F32)
            passed = (k > y) if way else (k < y)
            before[way] = jnp.where(passed, total[way], before[way])
    for way in range(2):
        pre_ref[way] = before[way]
    ahead, behind = total[0].astype(BF16), total[1].astype(BF16)
    for peer in range(8):
        send_ref[peer] = jnp.where(peer > z, ahead, behind)


def finish_mixer(
    place_ref,
    got_ref,
    pre_ref,
    local_ref,
    reads_ref,
    keys_ref,
    values_ref,
    rates_ref,
    valve_ref,
    reward_ref,
    gain_ref,
    projector_ref,
    send_ref,
):
    z = place_ref[1]
    state = [jnp.zeros((HEAD, WIDE), F32)] * 2
    for step in range(7):
        for way in range(2):
            k = 7 - step if way else step
            passed = (k > z) if way else (k < z)
            piece = got_ref[k]
            later = advanced(piece, state[way]) if step else piece[:, :WIDE].astype(F32)
            state[way] = jnp.where(passed, later, state[way])
    summed = 0.0
    for way in range(2):
        entering = advanced(pre_ref[way], state[way])
        summed = summed + local_ref[way, :, :WIDE]
        summed = summed + dot(local_ref[way, :, WIDE:], by_head(entering))
    off = summed - head_sums(summed) * (1.0 / HEAD)
    spread = head_sums(off * off) * (1.0 / HEAD)
    normed = off * lax.rsqrt(spread + GROUP_EPS) * gain_ref[...]
    keys = keys_ref[...].astype(F32)
    both = keys * sigmoid(rates_ref[0].astype(F32)) + keys * sigmoid(rates_ref[1].astype(F32))
    bonus = head_sums(reads_ref[...].astype(F32) * both * reward_ref[...])
    bonus = bonus * values_ref[...].astype(F32)
    mixed = ((normed + bonus) * valve_ref[...].astype(F32)).astype(BF16)
    share = jnp.dot(mixed, projector_ref[...], preferred_element_type=F32)
    send_ref[...] = share.astype(BF16).reshape(send_ref.shape)


def normed_rows(x, gain):
    off = x - jnp.mean(x, axis=-1, keepdims=True)
    spread = jnp.mean(off * off, axis=-1, keepdims=True)
    return off * lax.rsqrt(spread + NORM_EPS) * gain


def middle_rows(place_ref, got_ref, skip_ref, gain_ref, send_ref):
    summed = jnp.sum(got_ref[...].astype(F32), axis=0)
    mine = skip_ref[pl.ds(pl.multiple_of(place_ref[2] * 8, 8), 8), :]
    summed = summed + RESIDUAL_SCALE * mine.astype(F32)
    middle = normed_rows(summed, gain_ref[...]).astype(BF16)
    for peer in range(send_ref.shape[0]):
        send_ref[peer] = middle


def closing_rows(got_ref, middle_ref, gain_ref, out_ref):
    summed = jnp.sum(got_ref[...].astype(F32), axis=0)
    summed = summed + RESIDUAL_SCALE * middle_ref[0].astype(F32)
    out_ref[...] = normed_rows(summed, gain_ref[...]).astype(BF16)


def pack_weights(valve_ref, widen_ref, shrink_ref, send_ref):
    blank = jnp.zeros((valve_ref.shape[0], 2 * PART - UNITS), BF16)
    halves = []
    for lo in (0, PART):
        line = []
        for whole in (valve_ref[...], widen_ref[...], shrink_ref[...]):
            line.append(whole[:, lo : lo + PART])
            if lo:
                line.append(blank)
        halves.append(jnp.concatenate(line, axis=1))
    for peer in range(send_ref.shape[0]):
        send_ref[peer] = halves[peer % 2]


PLANE = 256
PARTS = D // PLANE


def feed_forward(rows_ref, weights_ref, out_ref, held_ref, arrived):
    copies = []
    for k in range(PARTS):
        rows = pl.ds(k * PLANE, PLANE)
        copies.append(
            pltpu.make_async_copy(weights_ref.at[rows], held_ref.at[rows], arrived.at[k])
        )
        copies[k].start()
    sums = 0.0
    for k in range(PARTS):
        copies[k].wait()
        rows = slice(k * PLANE, (k + 1) * PLANE)
        sums = sums + jnp.dot(
            rows_ref[:, rows], held_ref[rows, : 2 * PART], preferred_element_type=F32
        )
    gate, up = sums[:, :PART], sums[:, PART:]
    inner = (gate / (1.0 + jnp.exp(-gate)) * up).astype(BF16)
    for k in range(PARTS):
        rows = slice(k * PLANE, (k + 1) * PLANE)
        share = lax.dot_general(
            inner, held_ref[rows, 2 * PART :], (((1,), (1,)), ((), ())), preferred_element_type=F32
        )
        out_ref[:, :, rows] = share.astype(BF16).reshape(PEER_COUNT, 8, PLANE)


VMEM = pl.BlockSpec(memory_space=pltpu.VMEM)
SMEM = pl.BlockSpec(memory_space=pltpu.SMEM)


def shape(dims, kind=BF16):
    return pltpu.VMEM(dims, kind)


def near(*arrays):
    return [pltpu.with_memory_space_constraint(a, pltpu.VMEM) for a in arrays]


def cost(us):
    return pl.CostEstimate(flops=int(us * 2.0e8), transcendentals=0, bytes_accessed=0)


def whole(array):
    return pl.BlockSpec(array.shape, lambda *_: (0,) * array.ndim)


def exchanged(value, axis):
    return lax.all_to_all(value, axis, 0, 0, tiled=True)


def run_mixer_local(place, *args):
    return pl.pallas_call(
        mixer_local,
        grid=(1,),
        in_specs=[SMEM] + [whole(a) for a in args],
        out_specs=[VMEM] * 2,
        out_shape=[shape((8, HEAD, 4 * WIDE)), shape((2, TOK, 2 * WIDE), F32)],
        cost_estimate=cost(8),
        name="mixer_local",
    )(place, *args)


def run_combine_near(place, got):
    return pl.pallas_call(
        combine_near,
        in_specs=[SMEM, VMEM],
        out_specs=[VMEM] * 2,
        out_shape=[shape((8, HEAD, 2 * WIDE)), shape((2, HEAD, 2 * WIDE), F32)],
        cost_estimate=cost(3),
        name="combine_near",
    )(place, *near(got))


def run_finish_mixer(place, *args):
    return pl.pallas_call(
        finish_mixer,
        in_specs=[SMEM] + [VMEM] * (len(args)),
        out_specs=VMEM,
        out_shape=shape((8, 8, D)),
        cost_estimate=cost(4),
        name="finish_mixer",
    )(place, *near(*args))


def run_middle_rows(place, got, skip, gain, peers):
    return pl.pallas_call(
        middle_rows,
        in_specs=[SMEM] + [VMEM] * 3,
        out_specs=VMEM,
        out_shape=shape((peers, 8, D)),
        cost_estimate=cost(2),
        name="middle_rows",
    )(place, *near(got, skip, gain))


def run_feed_forward(rows, weights):
    return pl.pallas_call(
        feed_forward,
        in_specs=[VMEM, pl.BlockSpec(memory_space=pl.ANY)],
        out_specs=VMEM,
        out_shape=shape((PEER_COUNT, 8, D)),
        scratch_shapes=[
            pltpu.VMEM((D, 3 * PART), BF16),
            pltpu.SemaphoreType.DMA((PARTS,)),
        ],
        cost_estimate=cost(4),
        name="feed_forward",
    )(*near(rows), weights)


def run_closing_rows(got, middle, gain):
    return pl.pallas_call(
        closing_rows,
        in_specs=[VMEM] * 3,
        out_specs=VMEM,
        out_shape=jax.ShapeDtypeStruct((8, D), BF16),
        cost_estimate=cost(2),
        name="closing_rows",
    )(*near(got, middle, gain))


def shards(
    skip_stream_entering,
    reading_vectors,
    blender_lookup_labels,
    blender_payloads,
    blender_result_valve,
    fading_logits,
    amend_speed_logits,
    extra_log_fades,
    present_reward_factors,
    attender_scaling_vector,
    blender_result_projector,
    blender_scaling_vector,
    perceptron_valve_factors,
    perceptron_widen_factors,
    perceptron_shrink_factors,
    closing_scaling_vector,
):
    place = jnp.stack([lax.axis_index(Y), lax.axis_index("z"), lax.axis_index("tp")]).astype(
        jnp.int32
    )
    given = (perceptron_valve_factors, perceptron_widen_factors, perceptron_shrink_factors.T)
    packed = pl.pallas_call(
        pack_weights,
        grid=(1,),
        in_specs=[whole(a) for a in given],
        out_specs=VMEM,
        out_shape=shape((8, 32, 3 * PART)),
        cost_estimate=cost(2),
        name="pack_weights",
    )(*given)
    own = exchanged(packed, Y).reshape(PLANE, 3 * PART)
    sends, local = run_mixer_local(
        place,
        reading_vectors,
        blender_lookup_labels,
        blender_payloads,
        fading_logits,
        amend_speed_logits,
        extra_log_fades,
    )
    near_states = exchanged(sends, Y)
    weights = [lax.all_gather(own, "z", axis=0, tiled=True)]
    totals, before = run_combine_near(place, near_states)
    far_states = exchanged(totals, "z")
    shares = run_finish_mixer(
        place,
        far_states,
        before,
        local,
        reading_vectors,
        blender_lookup_labels,
        blender_payloads,
        amend_speed_logits,
        blender_result_valve,
        present_reward_factors.reshape(1, WIDE),
        attender_scaling_vector.reshape(1, WIDE),
        blender_result_projector,
    )
    shares = exchanged(shares, "tp")
    middle = run_middle_rows(
        place, shares, skip_stream_entering, blender_scaling_vector.reshape(1, D), PEER_COUNT
    )
    rows = exchanged(middle, PEERS).reshape(PEER_COUNT * 8, D)
    down = run_feed_forward(rows, weights[0])
    down = exchanged(down, PEERS)
    return run_closing_rows(down, middle, closing_scaling_vector.reshape(1, D))


def solution(mesh):
    finer = Mesh(mesh.devices.reshape(8, 4, 2, mesh.shape["tp"]), SP_TP)
    placed = (
        P(SP, None),
        P(SP, "tp"),
        P(SP, "tp"),
        P(SP, "tp"),
        P(SP, "tp"),
        P(None, SP, "tp"),
        P(None, SP, "tp"),
        P(None, "tp", SP),
        P("tp"),
        P("tp"),
        P("tp", None),
        P(),
        P(SP, "tp"),
        P(SP, "tp"),
        P("tp", SP),
        P(),
    )
    return jax.shard_map(
        shards, mesh=finer, in_specs=placed, out_specs=P(SP_TP, None), check_vma=False
    )
```

```python
import math

import jax
import jax.numpy as jnp
from jax import lax
from jax.experimental import pallas as pl
from jax.experimental.pallas import tpu as pltpu
from jax.sharding import Mesh
from jax.sharding import PartitionSpec as P

Y = ("yh", "yl")
SP = ("z", "yh", "yl")
SP_TP = SP + ("tp",)
PEERS = ("yl", "tp")

RESIDUAL_SCALE = 2.0**0.25
NORM_EPS = 1e-05
GROUP_EPS = 0.00064
KEY_EPS = 1e-06
TOK = 64
HEAD = 64
WIDE = 128
SUB = 16
UNITS = 704
PART = 384
PEER_COUNT = 16
D = 2048
F32 = jnp.float32
BF16 = jnp.bfloat16


def iota(shape, dim):
    return lax.broadcasted_iota(jnp.int32, shape, dim)


def split(x):
    high = x.astype(BF16)
    return high, (x - high.astype(F32)).astype(BF16)


def product(a, b, dims):
    (a_high, a_low), (b_high, b_low) = split(a), split(b)

    def part(one, two):
        return lax.dot_general(one, two, (dims, ((), ())), preferred_element_type=F32)

    return part(a_high, b_high) + (part(a_high, b_low) + part(a_low, b_high))


def dot(a, b):
    return product(a, b, ((1,), (0,)))


def dot_nt(a, b):
    return product(a, b, ((1,), (1,)))


def dot_tn(a, b):
    return product(a, b, ((0,), (0,)))


def chosen(picks, x, dims=((1,), (0,))):
    high, middle = split(x)
    low = (x - high.astype(F32) - middle.astype(F32)).astype(BF16)
    parts = [
        lax.dot_general(picks, part, (dims, ((), ())), preferred_element_type=F32)
        for part in (high, middle, low)
    ]
    return parts[0] + (parts[1] + parts[2])


def head_sums(x):
    high, low = split(x)
    ones = head_ones().astype(BF16)
    return jnp.dot(high, ones, preferred_element_type=F32) + jnp.dot(
        low, ones, preferred_element_type=F32
    )


def low_half(shape):
    return (iota(shape, len(shape) - 1) % WIDE) < HEAD


def by_head(x):
    low = low_half(x.shape)
    return jnp.concatenate([jnp.where(low, x, 0.0), jnp.where(low, 0.0, x)], axis=0)


def joined_heads(x):
    return x[:HEAD] + x[HEAD:]


def head_ones():
    return ((iota((WIDE, WIDE), 0) // HEAD) == (iota((WIDE, WIDE), 1) // HEAD)).astype(F32)


def head_eye():
    return (iota((HEAD, WIDE), 0) == iota((HEAD, WIDE), 1) % HEAD).astype(F32)


def sigmoid(x):
    return 1.0 / (1.0 + jnp.exp(-x))


def spread_heads(extra):
    lanes_of = (iota((2, WIDE), 1) // HEAD == iota((2, WIDE), 0)).astype(BF16)
    high, middle = split(extra)
    low = (extra - high.astype(F32) - middle.astype(F32)).astype(BF16)
    parts = [
        lax.dot_general(part, lanes_of, (((0,), (0,)), ((), ())), preferred_element_type=F32)
        for part in (high, middle, low)
    ]
    return parts[0] + (parts[1] + parts[2])


def unit_lower_inverse(a):
    row, col = iota((WIDE, WIDE), 0), iota((WIDE, WIDE), 1)
    eye = (row == col).astype(F32)
    near = jnp.where(row // 8 == col // 8, a, 0.0)
    second = dot(near, near)
    fourth = dot(second, second)
    inverse = eye - near + second - dot(near, second)
    inverse = inverse + dot(inverse, fourth)
    for size in (8, 16, 32):
        across = (row // (2 * size) == col // (2 * size)) & (row // size != col // size)
        inverse = inverse - dot(inverse, dot(jnp.where(across, a, 0.0), inverse))
    return inverse


def one_way(back, reads, unit, keys, values, log_decay, rate):
    refill, write = unit * rate, keys * rate
    row, col = iota((TOK, TOK), 0), iota((TOK, TOK), 1)
    reach = (col >= row) if back else (col <= row)
    upto = chosen(reach.astype(BF16), log_decay)
    ahead = upto - log_decay
    whole = upto[:1] if back else upto[TOK - 1 :]
    low = low_half((SUB, WIDE))
    first, second = [], []
    for block in range(TOK // SUB):
        rows = slice(block * SUB, (block + 1) * SUB)
        edge = (block + 1) * SUB - 1 if back else block * SUB
        start = ahead[edge : edge + 1]
        scale = jnp.exp(jnp.minimum(start - upto, 60.0))
        erase_keys, write_keys = refill * scale, write * scale
        erased = unit[rows] * jnp.exp(ahead[rows] - start)
        read = reads[rows] * jnp.exp(upto[rows] - start)
        first.append(
            dot_nt(
                jnp.concatenate([jnp.where(low, erased, 0.0), jnp.where(low, read, 0.0)], axis=0),
                jnp.concatenate([erase_keys, write_keys], axis=0),
            )
        )
        second.append(
            dot_nt(
                jnp.concatenate([jnp.where(low, 0.0, erased), jnp.where(low, 0.0, read)], axis=0),
                jnp.concatenate([write_keys, erase_keys], axis=0),
            )
        )
    row, col = iota((TOK, WIDE), 0), iota((TOK, WIDE), 1) % HEAD
    past = (col > row) if back else (col < row)
    seen = (col >= row) if back else (col <= row)
    low = low_half((TOK, WIDE))

    def pieces(kept, lo):
        one = jnp.concatenate([part[lo : lo + SUB] for part in first], axis=0)
        two = jnp.concatenate([part[lo : lo + SUB] for part in second], axis=0)
        one, two = jnp.where(kept, one, 0.0), jnp.where(kept, two, 0.0)
        same = jnp.concatenate([jnp.where(low, one, 0.0), jnp.where(low, 0.0, two)], axis=0)
        other = jnp.concatenate([jnp.where(low, 0.0, one), jnp.where(low, two, 0.0)], axis=0)
        return same, other

    erase_erase, erase_write = pieces(past, 0)
    read_erase, read_write = pieces(seen, SUB)
    straight = by_head(values)
    crossed = jnp.concatenate([straight[TOK:], straight[:TOK]], axis=0)
    asked = jnp.concatenate([dot(erase_write, crossed), by_head(unit * jnp.exp(ahead))], axis=1)
    erased = -dot(unit_lower_inverse(erase_erase), asked)
    out = dot(read_erase, erased) + jnp.concatenate(
        [dot(read_write, crossed), by_head(reads * jnp.exp(upto))], axis=1
    )
    left = jnp.exp(whole - upto)
    state = dot_tn(by_head(refill * left), erased)
    state = joined_heads(state) + jnp.concatenate(
        [
            joined_heads(dot_tn(by_head(write * left), straight)),
            head_eye() * jnp.exp(whole),
        ],
        axis=1,
    )
    return joined_heads(out), state


def mixer_local(reads_ref, keys_ref, values_ref, fades_ref, rates_ref, extra_ref, send_ref, out_ref):
    reads, keys = reads_ref[...].astype(F32), keys_ref[...].astype(F32)
    values = values_ref[...].astype(F32)
    unit = keys * lax.rsqrt(head_sums(keys * keys) + KEY_EPS)
    for way in range(2):
        log_decay = -math.exp(-0.5) * sigmoid(fades_ref[way].astype(F32))
        log_decay = log_decay + spread_heads(extra_ref[way])
        rate = sigmoid(rates_ref[way].astype(F32))
        out, state = one_way(way == 1, reads, unit, keys, values, log_decay, rate)
        out_ref[way] = out
        state = state.astype(BF16)
        for peer in range(send_ref.shape[0]):
            send_ref[peer, :, way * 2 * WIDE : (way + 1) * 2 * WIDE] = state


def advanced(piece, running):
    high, low = split(by_head(running))
    step = piece[:, WIDE:]
    if step.dtype == F32:
        moved = dot(step, by_head(running))
    else:
        moved = jnp.dot(step, high, preferred_element_type=F32)
        moved = moved + jnp.dot(step, low, preferred_element_type=F32)
    if running.shape[1] == WIDE:
        return moved + piece[:, :WIDE]
    return moved + jnp.concatenate([piece[:, :WIDE], jnp.zeros((HEAD, WIDE), F32)], axis=1)


def combine_near(got_ref, send_ref, pre_ref):
    y = lax.axis_index("yh") * 2 + lax.axis_index("yl")
    z = lax.axis_index("z")
    start = jnp.concatenate([jnp.zeros((HEAD, WIDE), F32), head_eye()], axis=1)
    total, before = [start, start], [start, start]
    for step in range(8):
        for way in range(2):
            k = 7 - step if way else step
            piece = got_ref[k, :, way * 2 * WIDE : (way + 1) * 2 * WIDE]
            total[way] = advanced(piece, total[way]) if step else piece.astype(F32)
            passed = (k > y) if way else (k < y)
            before[way] = jnp.where(passed, total[way], before[way])
    for way in range(2):
        pre_ref[way] = before[way]
    ahead, behind = total[0].astype(BF16), total[1].astype(BF16)
    for peer in range(8):
        send_ref[peer] = jnp.where(peer > z, ahead, behind)


def finish_mixer(
    got_ref,
    pre_ref,
    local_ref,
    reads_ref,
    keys_ref,
    values_ref,
    rates_ref,
    valve_ref,
    reward_ref,
    gain_ref,
    projector_ref,
    send_ref,
):
    z = lax.axis_index("z")
    state = [jnp.zeros((HEAD, WIDE), F32)] * 2
    for step in range(7):
        for way in range(2):
            k = 7 - step if way else step
            passed = (k > z) if way else (k < z)
            piece = got_ref[k]
            later = advanced(piece, state[way]) if step else piece[:, :WIDE].astype(F32)
            state[way] = jnp.where(passed, later, state[way])
    summed = 0.0
    for way in range(2):
        entering = advanced(pre_ref[way], state[way])
        summed = summed + local_ref[way, :, :WIDE]
        summed = summed + dot(local_ref[way, :, WIDE:], by_head(entering))
    off = summed - head_sums(summed) * (1.0 / HEAD)
    spread = head_sums(off * off) * (1.0 / HEAD)
    normed = off * lax.rsqrt(spread + GROUP_EPS) * gain_ref[...]
    keys = keys_ref[...].astype(F32)
    both = keys * sigmoid(rates_ref[0].astype(F32)) + keys * sigmoid(rates_ref[1].astype(F32))
    bonus = head_sums(reads_ref[...].astype(F32) * both * reward_ref[...])
    bonus = bonus * values_ref[...].astype(F32)
    mixed = ((normed + bonus) * valve_ref[...].astype(F32)).astype(BF16)
    share = jnp.dot(mixed, projector_ref[...], preferred_element_type=F32)
    send_ref[...] = share.astype(BF16).reshape(send_ref.shape)


def normed_rows(x, gain):
    off = x - jnp.mean(x, axis=-1, keepdims=True)
    spread = jnp.mean(off * off, axis=-1, keepdims=True)
    return off * lax.rsqrt(spread + NORM_EPS) * gain


def middle_rows(got_ref, skip_ref, gain_ref, send_ref):
    summed = jnp.sum(got_ref[...].astype(F32), axis=0)
    mine = skip_ref[pl.ds(pl.multiple_of(lax.axis_index("tp") * 8, 8), 8), :]
    summed = summed + RESIDUAL_SCALE * mine.astype(F32)
    middle = normed_rows(summed, gain_ref[...]).astype(BF16)
    for peer in range(send_ref.shape[0]):
        send_ref[peer] = middle


def closing_rows(got_ref, middle_ref, gain_ref, out_ref):
    summed = jnp.sum(got_ref[...].astype(F32), axis=0)
    summed = summed + RESIDUAL_SCALE * middle_ref[0].astype(F32)
    out_ref[...] = normed_rows(summed, gain_ref[...]).astype(BF16)


def pack_weights(valve_ref, widen_ref, shrink_ref, send_ref):
    blank = jnp.zeros((valve_ref.shape[0], 2 * PART - UNITS), BF16)
    halves = []
    for lo in (0, PART):
        line = []
        for whole in (valve_ref[...], widen_ref[...], shrink_ref[...]):
            line.append(whole[:, lo : lo + PART])
            if lo:
                line.append(blank)
        halves.append(jnp.concatenate(line, axis=1))
    for peer in range(send_ref.shape[0]):
        send_ref[peer] = halves[peer % 2]


PLANE = 256
PARTS = D // PLANE


def feed_forward(rows_ref, weights_ref, out_ref, held_ref, arrived):
    copies = []
    for k in range(PARTS):
        rows = pl.ds(k * PLANE, PLANE)
        copies.append(
            pltpu.make_async_copy(weights_ref.at[rows], held_ref.at[rows], arrived.at[k])
        )
        copies[k].start()
    sums = 0.0
    for k in range(PARTS):
        copies[k].wait()
        rows = slice(k * PLANE, (k + 1) * PLANE)
        sums = sums + jnp.dot(
            rows_ref[:, rows], held_ref[rows, : 2 * PART], preferred_element_type=F32
        )
    gate, up = sums[:, :PART], sums[:, PART:]
    inner = (gate / (1.0 + jnp.exp(-gate)) * up).astype(BF16)
    for k in range(PARTS):
        rows = slice(k * PLANE, (k + 1) * PLANE)
        share = lax.dot_general(
            inner, held_ref[rows, 2 * PART :], (((1,), (1,)), ((), ())), preferred_element_type=F32
        )
        out_ref[:, :, rows] = share.astype(BF16).reshape(PEER_COUNT, 8, PLANE)


VMEM = pl.BlockSpec(memory_space=pltpu.VMEM)
SMEM = pl.BlockSpec(memory_space=pltpu.SMEM)


def shape(dims, kind=BF16):
    return pltpu.VMEM(dims, kind)


def near(*arrays):
    return [pltpu.with_memory_space_constraint(a, pltpu.VMEM) for a in arrays]


def cost(us):
    return pl.CostEstimate(flops=int(us * 2.0e8), transcendentals=0, bytes_accessed=0)


def whole(array):
    return pl.BlockSpec(array.shape, lambda *_: (0,) * array.ndim)


def exchanged(value, axis):
    return lax.all_to_all(value, axis, 0, 0, tiled=True)


def run_mixer_local(*args):
    return pl.pallas_call(
        mixer_local,
        grid=(1,),
        in_specs=[whole(a) for a in args],
        out_specs=[VMEM] * 2,
        out_shape=[shape((8, HEAD, 4 * WIDE)), shape((2, TOK, 2 * WIDE), F32)],
        cost_estimate=cost(8),
        name="mixer_local",
    )(*args)


def run_combine_near(got):
    return pl.pallas_call(
        combine_near,
        in_specs=[VMEM],
        out_specs=[VMEM] * 2,
        out_shape=[shape((8, HEAD, 2 * WIDE)), shape((2, HEAD, 2 * WIDE), F32)],
        cost_estimate=cost(3),
        name="combine_near",
    )(*near(got))


def run_finish_mixer(*args):
    return pl.pallas_call(
        finish_mixer,
        in_specs=[VMEM] * len(args),
        out_specs=VMEM,
        out_shape=shape((8, 8, D)),
        cost_estimate=cost(4),
        name="finish_mixer",
    )(*near(*args))


def run_middle_rows(got, skip, gain, peers):
    return pl.pallas_call(
        middle_rows,
        in_specs=[VMEM] * 3,
        out_specs=VMEM,
        out_shape=shape((peers, 8, D)),
        cost_estimate=cost(2),
        name="middle_rows",
    )(*near(got, skip, gain))


def run_feed_forward(rows, weights):
    return pl.pallas_call(
        feed_forward,
        in_specs=[VMEM, pl.BlockSpec(memory_space=pl.ANY)],
        out_specs=VMEM,
        out_shape=shape((PEER_COUNT, 8, D)),
        scratch_shapes=[
            pltpu.VMEM((D, 3 * PART), BF16),
            pltpu.SemaphoreType.DMA((PARTS,)),
        ],
        cost_estimate=cost(4),
        name="feed_forward",
    )(*near(rows), weights)


def run_closing_rows(got, middle, gain):
    return pl.pallas_call(
        closing_rows,
        in_specs=[VMEM] * 3,
        out_specs=VMEM,
        out_shape=jax.ShapeDtypeStruct((8, D), BF16),
        cost_estimate=cost(2),
        name="closing_rows",
    )(*near(got, middle, gain))


def shards(
    skip_stream_entering,
    reading_vectors,
    blender_lookup_labels,
    blender_payloads,
    blender_result_valve,
    fading_logits,
    amend_speed_logits,
    extra_log_fades,
    present_reward_factors,
    attender_scaling_vector,
    blender_result_projector,
    blender_scaling_vector,
    perceptron_valve_factors,
    perceptron_widen_factors,
    perceptron_shrink_factors,
    closing_scaling_vector,
):
    given = (perceptron_valve_factors, perceptron_widen_factors, perceptron_shrink_factors.T)
    packed = pl.pallas_call(
        pack_weights,
        grid=(1,),
        in_specs=[whole(a) for a in given],
        out_specs=VMEM,
        out_shape=shape((8, 32, 3 * PART)),
        cost_estimate=cost(2),
        name="pack_weights",
    )(*given)
    own = exchanged(packed, Y).reshape(PLANE, 3 * PART)
    sends, local = run_mixer_local(
        reading_vectors,
        blender_lookup_labels,
        blender_payloads,
        fading_logits,
        amend_speed_logits,
        extra_log_fades,
    )
    near_states = exchanged(sends, Y)
    weights = [lax.all_gather(own, "z", axis=0, tiled=True)]
    totals, before = run_combine_near(near_states)
    far_states = exchanged(totals, "z")
    shares = run_finish_mixer(
        far_states,
        before,
        local,
        reading_vectors,
        blender_lookup_labels,
        blender_payloads,
        amend_speed_logits,
        blender_result_valve,
        present_reward_factors.reshape(1, WIDE),
        attender_scaling_vector.reshape(1, WIDE),
        blender_result_projector,
    )
    shares = exchanged(shares, "tp")
    middle = run_middle_rows(
        shares, skip_stream_entering, blender_scaling_vector.reshape(1, D), PEER_COUNT
    )
    rows = exchanged(middle, PEERS).reshape(PEER_COUNT * 8, D)
    down = run_feed_forward(rows, weights[0])
    down = exchanged(down, PEERS)
    return run_closing_rows(down, middle, closing_scaling_vector.reshape(1, D))


def solution(mesh):
    finer = Mesh(mesh.devices.reshape(8, 4, 2, mesh.shape["tp"]), SP_TP)
    placed = (
        P(SP, None),
        P(SP, "tp"),
        P(SP, "tp"),
        P(SP, "tp"),
        P(SP, "tp"),
        P(None, SP, "tp"),
        P(None, SP, "tp"),
        P(None, "tp", SP),
        P("tp"),
        P("tp"),
        P("tp", None),
        P(),
        P(SP, "tp"),
        P(SP, "tp"),
        P("tp", SP),
        P(),
    )
    return jax.shard_map(
        shards, mesh=finer, in_specs=placed, out_specs=P(SP_TP, None), check_vma=False
    )
```

```python
import math

import jax
import jax.numpy as jnp
from jax import lax
from jax.experimental import pallas as pl
from jax.experimental.pallas import tpu as pltpu
from jax.sharding import Mesh
from jax.sharding import PartitionSpec as P

Y = ("yh", "yl")
SP = ("z", "yh", "yl")
SP_TP = SP + ("tp",)
PEERS = ("yl", "tp")

RESIDUAL_SCALE = 2.0**0.25
NORM_EPS = 1e-05
GROUP_EPS = 0.00064
KEY_EPS = 1e-06
TOK = 64
HEAD = 64
WIDE = 128
SUB = 16
UNITS = 704
PART = 384
PEER_COUNT = 16
D = 2048
F32 = jnp.float32
BF16 = jnp.bfloat16


def iota(shape, dim):
    return lax.broadcasted_iota(jnp.int32, shape, dim)


def split(x):
    high = x.astype(BF16)
    return high, (x - high.astype(F32)).astype(BF16)


def product(a, b, dims):
    (a_high, a_low), (b_high, b_low) = split(a), split(b)

    def part(one, two):
        return lax.dot_general(one, two, (dims, ((), ())), preferred_element_type=F32)

    return part(a_high, b_high) + (part(a_high, b_low) + part(a_low, b_high))


def dot(a, b):
    return product(a, b, ((1,), (0,)))


def dot_nt(a, b):
    return product(a, b, ((1,), (1,)))


def dot_tn(a, b):
    return product(a, b, ((0,), (0,)))


def chosen(picks, x, dims=((1,), (0,))):
    high, middle = split(x)
    low = (x - high.astype(F32) - middle.astype(F32)).astype(BF16)
    parts = [
        lax.dot_general(picks, part, (dims, ((), ())), preferred_element_type=F32)
        for part in (high, middle, low)
    ]
    return parts[0] + (parts[1] + parts[2])


def head_sums(x):
    high, low = split(x)
    ones = head_ones().astype(BF16)
    return jnp.dot(high, ones, preferred_element_type=F32) + jnp.dot(
        low, ones, preferred_element_type=F32
    )


def low_half(shape):
    return (iota(shape, len(shape) - 1) % WIDE) < HEAD


def by_head(x):
    low = low_half(x.shape)
    return jnp.concatenate([jnp.where(low, x, 0.0), jnp.where(low, 0.0, x)], axis=0)


def joined_heads(x):
    return x[:HEAD] + x[HEAD:]


def head_ones():
    return ((iota((WIDE, WIDE), 0) // HEAD) == (iota((WIDE, WIDE), 1) // HEAD)).astype(F32)


def head_eye():
    return (iota((HEAD, WIDE), 0) == iota((HEAD, WIDE), 1) % HEAD).astype(F32)


def sigmoid(x):
    return 1.0 / (1.0 + jnp.exp(-x))


def spread_heads(extra):
    lanes_of = (iota((2, WIDE), 1) // HEAD == iota((2, WIDE), 0)).astype(BF16)
    high, middle = split(extra)
    low = (extra - high.astype(F32) - middle.astype(F32)).astype(BF16)
    parts = [
        lax.dot_general(part, lanes_of, (((0,), (0,)), ((), ())), preferred_element_type=F32)
        for part in (high, middle, low)
    ]
    return parts[0] + (parts[1] + parts[2])


def unit_lower_inverse(a):
    row, col = iota((WIDE, WIDE), 0), iota((WIDE, WIDE), 1)
    eye = (row == col).astype(F32)
    near = jnp.where(row // 8 == col // 8, a, 0.0)
    second = dot(near, near)
    fourth = dot(second, second)
    inverse = eye - near + second - dot(near, second)
    inverse = inverse + dot(inverse, fourth)
    for size in (8, 16, 32):
        across = (row // (2 * size) == col // (2 * size)) & (row // size != col // size)
        inverse = inverse - dot(inverse, dot(jnp.where(across, a, 0.0), inverse))
    return inverse


def one_way(back, reads, unit, keys, values, log_decay, rate):
    refill, write = unit * rate, keys * rate
    row, col = iota((TOK, TOK), 0), iota((TOK, TOK), 1)
    reach = (col >= row) if back else (col <= row)
    upto = chosen(reach.astype(BF16), log_decay)
    ahead = upto - log_decay
    whole = upto[:1] if back else upto[TOK - 1 :]
    low = low_half((SUB, WIDE))
    first, second = [], []
    for block in range(TOK // SUB):
        rows = slice(block * SUB, (block + 1) * SUB)
        edge = (block + 1) * SUB - 1 if back else block * SUB
        start = ahead[edge : edge + 1]
        scale = jnp.exp(jnp.minimum(start - upto, 60.0))
        erase_keys, write_keys = refill * scale, write * scale
        erased = unit[rows] * jnp.exp(ahead[rows] - start)
        read = reads[rows] * jnp.exp(upto[rows] - start)
        first.append(
            dot_nt(
                jnp.concatenate([jnp.where(low, erased, 0.0), jnp.where(low, read, 0.0)], axis=0),
                jnp.concatenate([erase_keys, write_keys], axis=0),
            )
        )
        second.append(
            dot_nt(
                jnp.concatenate([jnp.where(low, 0.0, erased), jnp.where(low, 0.0, read)], axis=0),
                jnp.concatenate([write_keys, erase_keys], axis=0),
            )
        )
    row, col = iota((TOK, WIDE), 0), iota((TOK, WIDE), 1) % HEAD
    past = (col > row) if back else (col < row)
    seen = (col >= row) if back else (col <= row)
    low = low_half((TOK, WIDE))

    def pieces(kept, lo):
        one = jnp.concatenate([part[lo : lo + SUB] for part in first], axis=0)
        two = jnp.concatenate([part[lo : lo + SUB] for part in second], axis=0)
        one, two = jnp.where(kept, one, 0.0), jnp.where(kept, two, 0.0)
        same = jnp.concatenate([jnp.where(low, one, 0.0), jnp.where(low, 0.0, two)], axis=0)
        other = jnp.concatenate([jnp.where(low, 0.0, one), jnp.where(low, two, 0.0)], axis=0)
        return same, other

    erase_erase, erase_write = pieces(past, 0)
    read_erase, read_write = pieces(seen, SUB)
    straight = by_head(values)
    crossed = jnp.concatenate([straight[TOK:], straight[:TOK]], axis=0)
    asked = jnp.concatenate([dot(erase_write, crossed), by_head(unit * jnp.exp(ahead))], axis=1)
    erased = -dot(unit_lower_inverse(erase_erase), asked)
    out = dot(read_erase, erased) + jnp.concatenate(
        [dot(read_write, crossed), by_head(reads * jnp.exp(upto))], axis=1
    )
    left = jnp.exp(whole - upto)
    state = dot_tn(by_head(refill * left), erased)
    state = joined_heads(state) + jnp.concatenate(
        [
            joined_heads(dot_tn(by_head(write * left), straight)),
            head_eye() * jnp.exp(whole),
        ],
        axis=1,
    )
    return joined_heads(out), state


def mixer_local(reads_ref, keys_ref, values_ref, fades_ref, rates_ref, extra_ref, send_ref, out_ref):
    reads, keys = reads_ref[...].astype(F32), keys_ref[...].astype(F32)
    values = values_ref[...].astype(F32)
    unit = keys * lax.rsqrt(head_sums(keys * keys) + KEY_EPS)
    for way in range(2):
        log_decay = -math.exp(-0.5) * sigmoid(fades_ref[way].astype(F32))
        log_decay = log_decay + spread_heads(extra_ref[way])
        rate = sigmoid(rates_ref[way].astype(F32))
        out, state = one_way(way == 1, reads, unit, keys, values, log_decay, rate)
        out_ref[way] = out
        state = state.astype(BF16)
        for peer in range(send_ref.shape[0]):
            send_ref[peer, :, way * 2 * WIDE : (way + 1) * 2 * WIDE] = state


def advanced(piece, running):
    high, low = split(by_head(running))
    step = piece[:, WIDE:]
    if step.dtype == F32:
        moved = dot(step, by_head(running))
    else:
        moved = jnp.dot(step, high, preferred_element_type=F32)
        moved = moved + jnp.dot(step, low, preferred_element_type=F32)
    if running.shape[1] == WIDE:
        return moved + piece[:, :WIDE]
    return moved + jnp.concatenate([piece[:, :WIDE], jnp.zeros((HEAD, WIDE), F32)], axis=1)


def combine_near(got_ref, send_ref, pre_ref):
    y = lax.axis_index("yh") * 2 + lax.axis_index("yl")
    z = lax.axis_index("z")
    start = jnp.concatenate([jnp.zeros((HEAD, WIDE), F32), head_eye()], axis=1)
    total, before = [start, start], [start, start]
    for step in range(8):
        for way in range(2):
            k = 7 - step if way else step
            piece = got_ref[k, :, way * 2 * WIDE : (way + 1) * 2 * WIDE]
            total[way] = advanced(piece, total[way]) if step else piece.astype(F32)
            passed = (k > y) if way else (k < y)
            before[way] = jnp.where(passed, total[way], before[way])
    for way in range(2):
        pre_ref[way] = before[way]
    ahead, behind = total[0].astype(BF16), total[1].astype(BF16)
    for peer in range(8):
        send_ref[peer] = jnp.where(peer > z, ahead, behind)


def finish_mixer(
    got_ref,
    pre_ref,
    local_ref,
    reads_ref,
    keys_ref,
    values_ref,
    rates_ref,
    valve_ref,
    reward_ref,
    gain_ref,
    projector_ref,
    send_ref,
    held_ref,
    arrived,
):
    copy = pltpu.make_async_copy(projector_ref, held_ref, arrived)
    copy.start()
    z = lax.axis_index("z")
    state = [jnp.zeros((HEAD, WIDE), F32)] * 2
    for step in range(7):
        for way in range(2):
            k = 7 - step if way else step
            passed = (k > z) if way else (k < z)
            piece = got_ref[k]
            later = advanced(piece, state[way]) if step else piece[:, :WIDE].astype(F32)
            state[way] = jnp.where(passed, later, state[way])
    summed = 0.0
    for way in range(2):
        entering = advanced(pre_ref[way], state[way])
        summed = summed + local_ref[way, :, :WIDE]
        summed = summed + dot(local_ref[way, :, WIDE:], by_head(entering))
    off = summed - head_sums(summed) * (1.0 / HEAD)
    spread = head_sums(off * off) * (1.0 / HEAD)
    normed = off * lax.rsqrt(spread + GROUP_EPS) * gain_ref[...]
    keys = keys_ref[...].astype(F32)
    both = keys * sigmoid(rates_ref[0].astype(F32)) + keys * sigmoid(rates_ref[1].astype(F32))
    bonus = head_sums(reads_ref[...].astype(F32) * both * reward_ref[...])
    bonus = bonus * values_ref[...].astype(F32)
    mixed = ((normed + bonus) * valve_ref[...].astype(F32)).astype(BF16)
    copy.wait()
    share = jnp.dot(mixed, held_ref[...], preferred_element_type=F32)
    send_ref[...] = share.astype(BF16).reshape(send_ref.shape)


def normed_rows(x, gain):
    off = x - jnp.mean(x, axis=-1, keepdims=True)
    spread = jnp.mean(off * off, axis=-1, keepdims=True)
    return off * lax.rsqrt(spread + NORM_EPS) * gain


def middle_rows(got_ref, skip_ref, gain_ref, send_ref):
    summed = jnp.sum(got_ref[...].astype(F32), axis=0)
    mine = skip_ref[pl.ds(pl.multiple_of(lax.axis_index("tp") * 8, 8), 8), :]
    summed = summed + RESIDUAL_SCALE * mine.astype(F32)
    middle = normed_rows(summed, gain_ref[...]).astype(BF16)
    for peer in range(send_ref.shape[0]):
        send_ref[peer] = middle


def closing_rows(got_ref, middle_ref, gain_ref, out_ref):
    summed = jnp.sum(got_ref[...].astype(F32), axis=0)
    summed = summed + RESIDUAL_SCALE * middle_ref[0].astype(F32)
    out_ref[...] = normed_rows(summed, gain_ref[...]).astype(BF16)


def pack_weights(valve_ref, widen_ref, shrink_ref, send_ref):
    blank = jnp.zeros((valve_ref.shape[0], 2 * PART - UNITS), BF16)
    halves = []
    for lo in (0, PART):
        line = []
        for whole in (valve_ref[...], widen_ref[...], shrink_ref[...]):
            line.append(whole[:, lo : lo + PART])
            if lo:
                line.append(blank)
        halves.append(jnp.concatenate(line, axis=1))
    for peer in range(send_ref.shape[0]):
        send_ref[peer] = halves[peer % 2]


PLANE = 256
PARTS = D // PLANE


def feed_forward(rows_ref, weights_ref, out_ref, held_ref, arrived):
    copies = []
    for k in range(PARTS):
        rows = pl.ds(k * PLANE, PLANE)
        copies.append(
            pltpu.make_async_copy(weights_ref.at[rows], held_ref.at[rows], arrived.at[k])
        )
        copies[k].start()
    sums = 0.0
    for k in range(PARTS):
        copies[k].wait()
        rows = slice(k * PLANE, (k + 1) * PLANE)
        sums = sums + jnp.dot(
            rows_ref[:, rows], held_ref[rows, : 2 * PART], preferred_element_type=F32
        )
    gate, up = sums[:, :PART], sums[:, PART:]
    inner = (gate / (1.0 + jnp.exp(-gate)) * up).astype(BF16)
    for k in range(PARTS):
        rows = slice(k * PLANE, (k + 1) * PLANE)
        share = lax.dot_general(
            inner, held_ref[rows, 2 * PART :], (((1,), (1,)), ((), ())), preferred_element_type=F32
        )
        out_ref[:, :, rows] = share.astype(BF16).reshape(PEER_COUNT, 8, PLANE)


VMEM = pl.BlockSpec(memory_space=pltpu.VMEM)
SMEM = pl.BlockSpec(memory_space=pltpu.SMEM)


def shape(dims, kind=BF16):
    return pltpu.VMEM(dims, kind)


def near(*arrays):
    return [pltpu.with_memory_space_constraint(a, pltpu.VMEM) for a in arrays]


def cost(us):
    return pl.CostEstimate(flops=int(us * 2.0e8), transcendentals=0, bytes_accessed=0)


def whole(array):
    return pl.BlockSpec(array.shape, lambda *_: (0,) * array.ndim)


def exchanged(value, axis):
    return lax.all_to_all(value, axis, 0, 0, tiled=True)


def run_mixer_local(*args):
    return pl.pallas_call(
        mixer_local,
        grid=(1,),
        in_specs=[whole(a) for a in args],
        out_specs=[VMEM] * 2,
        out_shape=[shape((8, HEAD, 4 * WIDE)), shape((2, TOK, 2 * WIDE), F32)],
        cost_estimate=cost(8),
        compiler_params=pltpu.CompilerParams(vmem_limit_bytes=66_200_000),
        name="mixer_local",
    )(*args)


def run_combine_near(got):
    return pl.pallas_call(
        combine_near,
        in_specs=[VMEM],
        out_specs=[VMEM] * 2,
        out_shape=[shape((8, HEAD, 2 * WIDE)), shape((2, HEAD, 2 * WIDE), F32)],
        cost_estimate=cost(3),
        name="combine_near",
    )(*near(got))


def run_finish_mixer(*args):
    *args, projector = args
    return pl.pallas_call(
        finish_mixer,
        in_specs=[VMEM] * len(args) + [pl.BlockSpec(memory_space=pl.ANY)],
        out_specs=VMEM,
        out_shape=shape((8, 8, D)),
        scratch_shapes=[pltpu.VMEM((WIDE, D), BF16), pltpu.SemaphoreType.DMA(())],
        cost_estimate=cost(4),
        name="finish_mixer",
    )(*near(*args), projector)


def run_middle_rows(got, skip, gain, peers):
    return pl.pallas_call(
        middle_rows,
        in_specs=[VMEM] * 3,
        out_specs=VMEM,
        out_shape=shape((peers, 8, D)),
        cost_estimate=cost(2),
        name="middle_rows",
    )(*near(got, skip, gain))


def run_feed_forward(rows, weights):
    return pl.pallas_call(
        feed_forward,
        in_specs=[VMEM, pl.BlockSpec(memory_space=pl.ANY)],
        out_specs=VMEM,
        out_shape=shape((PEER_COUNT, 8, D)),
        scratch_shapes=[
            pltpu.VMEM((D, 3 * PART), BF16),
            pltpu.SemaphoreType.DMA((PARTS,)),
        ],
        cost_estimate=cost(4),
        name="feed_forward",
    )(*near(rows), weights)


def run_closing_rows(got, middle, gain):
    return pl.pallas_call(
        closing_rows,
        in_specs=[VMEM] * 3,
        out_specs=VMEM,
        out_shape=jax.ShapeDtypeStruct((8, D), BF16),
        cost_estimate=cost(2),
        name="closing_rows",
    )(*near(got, middle, gain))


def shards(
    skip_stream_entering,
    reading_vectors,
    blender_lookup_labels,
    blender_payloads,
    blender_result_valve,
    fading_logits,
    amend_speed_logits,
    extra_log_fades,
    present_reward_factors,
    attender_scaling_vector,
    blender_result_projector,
    blender_scaling_vector,
    perceptron_valve_factors,
    perceptron_widen_factors,
    perceptron_shrink_factors,
    closing_scaling_vector,
):
    given = (perceptron_valve_factors, perceptron_widen_factors, perceptron_shrink_factors.T)
    packed = pl.pallas_call(
        pack_weights,
        grid=(1,),
        in_specs=[whole(a) for a in given],
        out_specs=VMEM,
        out_shape=shape((8, 32, 3 * PART)),
        cost_estimate=cost(2),
        name="pack_weights",
    )(*given)
    own = exchanged(packed, Y).reshape(PLANE, 3 * PART)
    sends, local = run_mixer_local(
        reading_vectors,
        blender_lookup_labels,
        blender_payloads,
        fading_logits,
        amend_speed_logits,
        extra_log_fades,
    )
    near_states = exchanged(sends, Y)
    weights = [lax.all_gather(own, "z", axis=0, tiled=True)]
    totals, before = run_combine_near(near_states)
    far_states = exchanged(totals, "z")
    shares = run_finish_mixer(
        far_states,
        before,
        local,
        reading_vectors,
        blender_lookup_labels,
        blender_payloads,
        amend_speed_logits,
        blender_result_valve,
        present_reward_factors.reshape(1, WIDE),
        attender_scaling_vector.reshape(1, WIDE),
        blender_result_projector,
    )
    shares = exchanged(shares, "tp")
    middle = run_middle_rows(
        shares, skip_stream_entering, blender_scaling_vector.reshape(1, D), PEER_COUNT
    )
    rows = exchanged(middle, PEERS).reshape(PEER_COUNT * 8, D)
    down = run_feed_forward(rows, weights[0])
    down = exchanged(down, PEERS)
    return run_closing_rows(down, middle, closing_scaling_vector.reshape(1, D))


def solution(mesh):
    finer = Mesh(mesh.devices.reshape(8, 4, 2, mesh.shape["tp"]), SP_TP)
    placed = (
        P(SP, None),
        P(SP, "tp"),
        P(SP, "tp"),
        P(SP, "tp"),
        P(SP, "tp"),
        P(None, SP, "tp"),
        P(None, SP, "tp"),
        P(None, "tp", SP),
        P("tp"),
        P("tp"),
        P("tp", None),
        P(),
        P(SP, "tp"),
        P(SP, "tp"),
        P("tp", SP),
        P(),
    )
    return jax.shard_map(
        shards, mesh=finer, in_specs=placed, out_specs=P(SP_TP, None), check_vma=False
    )
```
